32 devices in a mesh: fs: 8 (over z, core), tp: 4 (over y, x).
Axes of the slice: x: 2, y: 2, z: 4, core: 2. Of those that a mesh axis runs over, the one named last changes fastest.
Arguments:
- latent: bfloat16 [16384, 1024], P('fs'), may hold values from -6 to 6
- key_cotangent: bfloat16 [16384, 512], P('fs', 'tp'), may hold values from -0.046875 to 0.046875
- value_cotangent: bfloat16 [16384, 512], P('fs', 'tp'), may hold values from -0.046875 to 0.046875
- key_weight: float32 [1024, 512], P('fs', 'tp'), may hold values from -50 to 50
- value_weight: float32 [1024, 512], P('fs', 'tp'), may hold values from -50 to 50
- key_projector: bfloat16 [1024, 256], replicated, may hold values from -0.1875 to 0.1875
- value_projector: bfloat16 [1024, 256], replicated, may hold values from -0.1875 to 0.1875
- key_first: float32 [256, 512], P(None, 'tp'), may hold values from -6 to 6
- key_second: float32 [256, 512], P(None, 'tp'), may hold values from 0.3 to 3
- value_first: float32 [256, 512], P(None, 'tp'), may hold values from -6 to 6
- value_second: float32 [256, 512], P(None, 'tp'), may hold values from 0.3 to 3
Outputs:
- key_renewed: float32 [1024, 512], P('fs', 'tp')
- value_renewed: float32 [1024, 512], P('fs', 'tp')
- key_step: float32 [1024, 512], P('fs', 'tp')
- value_step: float32 [1024, 512], P('fs', 'tp')
- key_first_new: float32 [256, 512], P(None, 'tp')
- key_second_new: float32 [256, 512], P(None, 'tp')
- value_first_new: float32 [256, 512], P(None, 'tp')
- value_second_new: float32 [256, 512], P(None, 'tp')
- key_copy: bfloat16 [1024, 512], P(None, 'tp')
- value_copy: bfloat16 [1024, 512], P(None, 'tp')
The draws below stay inside these ranges and needn't reach their ends.
All inputs are finite; a program needn't handle non-finite values.
Results may differ from the reference program's by a relative error of at most 0.015.
Values may be sent and summed in bfloat16 or wider, within the bound.
A program may use at most 64 MiB of HBM per device.

```python
import math
import jax
import jax.numpy as jnp
from jax import lax

LATENT_WIDTH = 1024
KEY_FEATURES = 128
VALUE_FEATURES = 128
FACTOR_RANK = 256
ATTENTION_HEADS = 4
TOKEN_COUNT = 16384
KEY_COLS = 512
VALUE_COLS = 512


def draw_weight_common(key, row_total, col_total):
    row_place = jnp.arange(row_total, dtype=jnp.float32) / row_total
    col_place = jnp.arange(col_total, dtype=jnp.float32) / col_total
    keys = jax.random.split(key, 3)
    row_scale = 10.0 ** row_place
    col_scale = 10.0 ** col_place
    values = jnp.clip(jax.random.normal(keys[2], (row_total, col_total), jnp.float32), -5.0, 5.0)
    return (values * jnp.sqrt(row_scale[:, None] * col_scale[None, :])).astype(jnp.float32)


def draw_key_weight(key, part):
    return draw_weight_common(jax.random.fold_in(key, 11), LATENT_WIDTH, ATTENTION_HEADS * KEY_FEATURES)


def draw_value_weight(key, part):
    return draw_weight_common(jax.random.fold_in(key, 23), LATENT_WIDTH, ATTENTION_HEADS * VALUE_FEATURES)


def strengthened(entries, key, source, target, shards_of, factor):
    owner, partner = [(jnp.arange(entries.shape[position]) // (entries.shape[position] // shards_of)).reshape([-1 if axis == position else 1 for axis in range(entries.ndim)]) for position in (source, target)]
    chosen = jax.random.permutation(key, shards_of)[partner]
    strong = (owner == chosen) | (owner == (partner + shards_of // 2) % shards_of)
    return jnp.where(strong, factor * entries, entries)


def levels(rng, extent, shards, smallest, top_value):
    gain, own = 1.0, jax.random.fold_in(rng, 6)
    for axis_at, parts in shards:
        heights = jnp.exp(jax.random.uniform(jax.random.fold_in(own, axis_at), (parts,), jnp.float32, smallest / len(shards), top_value / len(shards)))
        gain = gain * jnp.repeat(heights, extent[axis_at] // parts).reshape([-1 if axis == axis_at else 1 for axis in range(len(extent))])
    return gain


def noise(stream_key, shape, spread, reach, cuts=(), kind=jnp.bfloat16):
    entries = jax.random.normal(stream_key, shape, jnp.float32) * spread
    if len(cuts) > 0:
        entries = levels(stream_key, shape, cuts, -0.22, 0.18) * entries
    return jnp.clip(entries, min=-reach, max=reach).astype(kind)


def heavy_noise(own_key, extent, scale, most, pieces, heavy, held_as=jnp.bfloat16):
    array = scale * jax.random.normal(own_key, extent, jnp.float32)
    if pieces:
        array = array * levels(own_key, extent, pieces, -0.22, 0.18)
    return jnp.clip(strengthened(array, jax.random.fold_in(own_key, 3), *heavy), -most, most).astype(held_as)


def setup_inputs(seed: int = 0) -> dict:
    splits = jax.random.split(jax.random.key(seed), 12)
    return {
        "latent": heavy_noise(splits[0], (TOKEN_COUNT, LATENT_WIDTH), 1.0, 6.0, ((0, 8),), (0, 1, 8, 2.0)),
        "key_cotangent": noise(splits[1], (TOKEN_COUNT, KEY_COLS), (1.0 / TOKEN_COUNT ** 0.5), 0.046875, ((0, 8), (1, 4))),
        "value_cotangent": noise(splits[2], (TOKEN_COUNT, VALUE_COLS), (1.0 / TOKEN_COUNT ** 0.5), 0.046875, ((0, 8), (1, 4))),
        "key_weight": draw_key_weight(jax.random.fold_in(splits[11], 71), 0),
        "value_weight": draw_value_weight(jax.random.fold_in(splits[11], 71), 0),
        "key_projector": noise(splits[5], (LATENT_WIDTH, FACTOR_RANK), LATENT_WIDTH ** -0.5, 0.1875),
        "value_projector": noise(splits[6], (LATENT_WIDTH, FACTOR_RANK), LATENT_WIDTH ** -0.5, 0.1875),
        "key_first": noise(splits[7], (FACTOR_RANK, KEY_COLS), 1.0, 6.0, ((1, 4),), jnp.float32),
        "key_second": jnp.clip(jnp.exp(math.log(3.0) - 2.3025851 * jax.random.uniform(splits[8], (FACTOR_RANK, KEY_COLS), jnp.float32) ** levels(splits[8], (FACTOR_RANK, KEY_COLS), ((1, 4),), -0.2, 0.2)), 0.3, 3.0),
        "value_first": noise(splits[9], (FACTOR_RANK, VALUE_COLS), 1.0, 6.0, ((1, 4),), jnp.float32),
        "value_second": jnp.clip(jnp.exp(math.log(3.0) - 2.3025851 * jax.random.uniform(splits[10], (FACTOR_RANK, VALUE_COLS), jnp.float32) ** levels(splits[10], (FACTOR_RANK, VALUE_COLS), ((1, 4),), -0.2, 0.2)), 0.3, 3.0),
    }


EPSILON = 1e-08
FIRST_DECAY = 0.7
SECOND_DECAY = 0.8
LEARN_RATE = 0.2

def update(latent, weight, factor, cotangent, first_moment, second):
    reduced = jnp.dot(latent.astype(jnp.float32), factor.astype(jnp.float32), precision=lax.Precision.HIGHEST)
    projected = jnp.dot(reduced.T, cotangent.astype(jnp.float32), precision=lax.Precision.HIGHEST)
    first_new = FIRST_DECAY * first_moment + (1.0 - FIRST_DECAY) * projected
    second_new = SECOND_DECAY * second + (1.0 - SECOND_DECAY) * projected * projected
    normalized = first_new / (jnp.sqrt(second_new) + EPSILON)
    direction = jnp.dot(factor.astype(jnp.float32), normalized, precision=lax.Precision.HIGHEST)
    step_scale = LEARN_RATE * jnp.sqrt(jnp.mean(weight * weight))
    weight_step = step_scale * direction
    renewed = weight - weight_step
    return (renewed, weight_step, first_new, second_new, renewed.astype(jnp.bfloat16))

def reference(latent, key_cotangent, value_cotangent, key_weight, value_weight, key_projector, value_projector, key_first, key_second, value_first, value_second):
    key_out = update(latent, key_weight, key_projector, key_cotangent, key_first, key_second)
    value_out = update(latent, value_weight, value_projector, value_cotangent, value_first, value_second)
    return (key_out[0], value_out[0], key_out[1], value_out[1], key_out[2], key_out[3], value_out[2], value_out[3], key_out[4], value_out[4])
```

```python
import functools

import jax
import jax.numpy as jnp
from jax import lax
from jax.experimental import pallas as pl
from jax.experimental.pallas import tpu as pltpu
from jax.sharding import PartitionSpec as P

EPSILON = 1e-08
FIRST_DECAY = 0.7
SECOND_DECAY = 0.8
LEARN_RATE = 0.2
CHUNKS = 4
BARRIER_CHUNK = 3
MESH = pl.DeviceIdType.MESH
HBM = pl.BlockSpec(memory_space=pltpu.MemorySpace.HBM)
VMEM = pl.BlockSpec(memory_space=pltpu.MemorySpace.VMEM)


def exchange_kernel(
    n,
    m,
    latent,
    key_cot,
    value_cot,
    key_weight,
    value_weight,
    key_proj,
    value_proj,
    key_first,
    key_second,
    value_first,
    value_second,
    gathered,
    weights,
    squares,
    weight_v,
    proj_v,
    moment_v,
    latent_v,
    cot_v,
    cot_t,
    reduced,
    partial,
    joined,
    received,
    tp_squares,
    load_sem,
    latent_sem,
    t_send,
    t_recv,
    s_send,
    s_recv,
    c_send,
    c_recv,
    rs_send,
    rs_recv,
    ag_send,
    ag_recv,
    p_send,
    p_recv,
    x_send,
    x_recv,
    w_send,
    w_recv,
    r_send,
    f_send,
    f_recv,
):
    me = lax.axis_index("fs")
    mine = lax.axis_index("tp")
    core = lax.rem(me, 2)
    chip = lax.div(me, 2)
    partner = me + 1 - 2 * core
    half = n // 2
    tokens, width = latent.shape
    step = width // CHUNKS
    rank = key_proj.shape[1]
    cols = key_cot.shape[1]
    piece = gathered.shape[1]
    f32, bf16 = jnp.float32, jnp.bfloat16

    def load(src, dst, sem):
        pltpu.make_async_copy(src, dst, sem).start()

    def landed(ref, sem):
        pltpu.make_async_copy(ref, ref, sem).wait()

    load(key_cot, cot_v.at[0], load_sem.at[0])
    load(value_cot, cot_v.at[1], load_sem.at[0])
    load(key_weight, weight_v.at[0], load_sem.at[1])
    load(value_weight, weight_v.at[1], load_sem.at[1])
    for c in range(CHUNKS):
        load(latent.at[:, pl.ds(c * step, step)], latent_v.at[c], latent_sem.at[c])
    load(key_proj, proj_v.at[0], load_sem.at[2])
    load(value_proj, proj_v.at[1], load_sem.at[2])
    load(key_first, moment_v.at[0], load_sem.at[3])
    load(key_second, moment_v.at[1], load_sem.at[3])
    load(value_first, moment_v.at[2], load_sem.at[3])
    load(value_second, moment_v.at[3], load_sem.at[3])

    barrier = pltpu.get_barrier_semaphore()
    for d in range(1, n):
        pl.semaphore_signal(
            barrier, inc=1, device_id={"fs": lax.rem(me + d, n)}, device_id_type=MESH
        )
    for d in range(1, m):
        pl.semaphore_signal(
            barrier, inc=1, device_id={"tp": lax.rem(mine + d, m)}, device_id_type=MESH
        )

    def remote(src, dst, send_sem, recv_sem, where):
        return pltpu.make_async_remote_copy(
            src_ref=src,
            dst_ref=dst,
            send_sem=send_sem,
            recv_sem=recv_sem,
            device_id=where,
            device_id_type=MESH,
        )

    def send(src, dst, send_sem, recv_sem, where):
        remote(src, dst, send_sem, recv_sem, where).start()

    def arrived(ref, sem):
        remote(ref, ref, sem, sem, {"fs": partner}).wait_recv()

    def left(ref, sem):
        remote(ref, ref, sem, sem, {"fs": partner}).wait_send()

    side = lax.div(chip, (half + 1) // 2)

    def far_first(k):
        down = half - 1 - k
        down = down - lax.div(chip - down + half, half)
        up = k + lax.div(k - chip + half, half)
        return down + side * (up - down)

    def near_first(k):
        return far_first(half - 2 - k)

    def direct(target):
        inner = (target > 0) & (target < half - 1)
        low = (target == 0) & (chip == 1)
        high = (target == half - 1) & (chip == half - 2)
        return inner | low | high

    def spread(shard):
        for k in range(half - 1):
            target = far_first(k)

            @pl.when(direct(target))
            def _():
                send(
                    weights.at[shard],
                    weights.at[shard],
                    w_send,
                    w_recv.at[shard],
                    {"fs": 2 * target},
                )

    with jax.named_scope("cot"):
        landed(cot_v, load_sem.at[0])
    for i in range(2):
        cot_t[pl.ds(i * cols, cols), :] = cot_v[i].T
    landed(weight_v, load_sem.at[1])
    for i in range(2):
        w = weight_v[i]
        weights[me, i] = w.astype(bf16)
        tp_squares[mine, pl.ds(i, 1), :] = jnp.sum(w * w, axis=0, keepdims=True)

    for c in range(CHUNKS):
        if c == BARRIER_CHUNK:
            with jax.named_scope("bar"):
                pl.semaphore_wait(barrier, n - 1 + m - 1)
            for d in range(1, m):
                send(
                    tp_squares.at[mine],
                    tp_squares.at[mine],
                    t_send,
                    t_recv,
                    {"tp": lax.rem(mine + d, m)},
                )
            send(weights.at[me], weights.at[me], x_send, x_recv, {"fs": partner})

            @pl.when(core == 0)
            def _():
                spread(me)

        with jax.named_scope(f"lat{c}"):
            landed(latent_v.at[c], latent_sem.at[c])
        reduced[:, pl.ds(c * step, step)] = jnp.dot(
            cot_t[...], latent_v[c], preferred_element_type=f32
        ).astype(bf16)
    landed(proj_v, load_sem.at[2])
    totals = [
        jnp.dot(
            reduced[pl.ds(i * cols, cols), :], proj_v[i], preferred_element_type=f32
        ).T
        for i in range(2)
    ]

    def spread_squares():
        for_all = [lax.rem(mine + d, m) for d in range(1, m)]
        arrived(tp_squares.at[pl.ds(0, len(for_all))], t_recv)
        squares[me] = jnp.sum(tp_squares[...], axis=0)
        for d in range(1, n):
            send(
                squares.at[me],
                squares.at[me],
                s_send,
                s_recv,
                {"fs": lax.rem(me + d, n)},
            )

    @pl.when(core == 0)
    def _():
        for i in range(2):
            partial[pl.ds(i * rank, rank), :] = totals[i].astype(bf16)
        send(partial, joined, c_send, c_recv, {"fs": partner})
        with jax.named_scope("xw"):
            arrived(weights.at[partner], x_recv)
        spread(partner)
        with jax.named_scope("tpsq"):
            spread_squares()
        for part in range(2):
            for k in range(half - 1):
                source = 2 * near_first(k) + part
                with jax.named_scope(f"w{part}{k}"):
                    arrived(weights.at[source], w_recv.at[source])
                for end, next_to_end in ((0, 1), (half - 1, half - 2)):

                    @pl.when((chip == next_to_end) & (lax.div(source, 2) != end))
                    def _():
                        send(
                            weights.at[source],
                            weights.at[source],
                            r_send,
                            w_recv.at[source],
                            {"fs": 2 * end},
                        )

                send(
                    weights.at[source],
                    weights.at[source],
                    f_send,
                    f_recv,
                    {"fs": partner},
                )
        with jax.named_scope("final"):
            arrived(gathered, p_recv)
        left(partial, c_send)
        for c in range(half):
            others = [t for t in range(half) if t != c]
            count = sum(
                0 < t < half - 1
                or (t == 0 and c == 1)
                or (t == half - 1 and c == half - 2)
                for t in others
            )
            ends = (0, 1), (half - 1, half - 2)
            relays = sum(t != end for end, near in ends if near == c for t in others)

            @pl.when(chip == c)
            def _():
                if count:
                    left(weights.at[pl.ds(0, 2 * count)], w_send)
                if relays:
                    left(weights.at[pl.ds(0, 2 * relays)], r_send)

        left(weights.at[pl.ds(0, n - 2)], f_send)

    @pl.when(core == 1)
    def _():
        with jax.named_scope("join"):
            arrived(joined, c_recv)
        for i in range(2):
            part = pl.ds(i * rank, rank)
            partial[part, :] = (totals[i] + joined[part, :].astype(f32)).astype(bf16)
        for k in range(half - 1):
            target = far_first(k)
            send(
                partial.at[pl.ds(target * piece, piece)],
                received.at[lax.rem(target - chip + half, half) - 1],
                rs_send,
                rs_recv,
                {"fs": 2 * target + 1},
            )
        with jax.named_scope("tpsq"):
            spread_squares()
        with jax.named_scope("rs"):
            arrived(received, rs_recv)
        own = partial[pl.ds(pl.multiple_of(chip * piece, piece), piece), :]
        gathered[chip] = (
            own.astype(f32) + jnp.sum(received[...].astype(f32), axis=0)
        ).astype(bf16)
        for k in range(half - 1):
            send(
                gathered.at[chip],
                gathered.at[chip],
                ag_send,
                ag_recv.at[chip],
                {"fs": 2 * far_first(k) + 1},
            )
        send(gathered.at[chip], gathered.at[chip], p_send, p_recv, {"fs": partner})
        for k in range(half - 1):
            source = near_first(k)
            with jax.named_scope(f"ag{k}"):
                arrived(gathered.at[source], ag_recv.at[source])
            send(
                gathered.at[source],
                gathered.at[source],
                p_send,
                p_recv,
                {"fs": partner},
            )
        with jax.named_scope("xw"):
            arrived(weights.at[partner], x_recv)
        with jax.named_scope("fw"):
            arrived(weights.at[pl.ds(0, n - 2)], f_recv)
        left(received, rs_send)
        left(gathered.at[pl.ds(0, half - 1)], ag_send)
        with jax.named_scope("psend"):
            left(gathered, p_send)

    with jax.named_scope("sq"):
        arrived(squares.at[pl.ds(0, n - 1)], s_recv)
    left(squares.at[pl.ds(0, n - 1)], s_send)
    left(tp_squares.at[pl.ds(0, m - 1)], t_send)
    left(weights.at[me], x_send)
    landed(moment_v, load_sem.at[3])


def update_kernel(n, entries, *refs):
    gathered, weights, squares, weight_v, proj_v, moment_v = refs[:6]
    outs, (small, moment, copied), sems = refs[6:16], refs[16:19], refs[19]
    me = lax.axis_index("fs")
    f32, bf16 = jnp.float32, jnp.bfloat16
    rows, cols = weight_v.shape[1:]
    rank = moment_v.shape[1]

    def store(src, out, sem):
        pltpu.make_async_copy(src, outs[out], sems.at[sem]).start()

    both = gathered[...].astype(f32).reshape(2 * rank, cols)
    normalized = []
    for i in range(2):
        projected = both[i * rank : (i + 1) * rank]
        first_new = FIRST_DECAY * moment_v[2 * i] + (1.0 - FIRST_DECAY) * projected
        second_new = (
            SECOND_DECAY * moment_v[2 * i + 1]
            + (1.0 - SECOND_DECAY) * projected * projected
        )
        moment[2 * i] = first_new
        moment[2 * i + 1] = second_new
        store(moment.at[2 * i], 4 + 2 * i, 1)
        store(moment.at[2 * i + 1], 5 + 2 * i, 1)
        normalized.append((first_new / (jnp.sqrt(second_new) + EPSILON)).astype(bf16))
    tile = jnp.sum(squares[...], axis=0)
    for i in range(2):
        total = jnp.sum(tile[i : i + 1], keepdims=True)
        scale = LEARN_RATE * jnp.sqrt(total / entries)
        every = scale * jnp.dot(proj_v[i], normalized[i], preferred_element_type=f32)
        held = weights[:, i].astype(f32).reshape(n * rows, cols)
        copied[i] = (held - every).astype(bf16)
        store(copied.at[i], 8 + i, 2)
        own = proj_v[i, pl.ds(pl.multiple_of(me * rows, rows), rows), :]
        own_step = scale * jnp.dot(own, normalized[i], preferred_element_type=f32)
        small[2 + i] = own_step
        small[i] = weight_v[i] - own_step
        store(small.at[2 + i], 2 + i, 0)
        store(small.at[i], i, 0)
    for sem, ref in enumerate((small, moment, copied)):
        pltpu.make_async_copy(ref, ref, sems.at[sem]).wait()


def solution(mesh):
    n, m = mesh.shape["fs"], mesh.shape["tp"]

    def body(
        latent,
        key_cot,
        value_cot,
        key_weight,
        value_weight,
        key_proj,
        value_proj,
        key_first,
        key_second,
        value_first,
        value_second,
    ):
        f32, bf16 = jnp.float32, jnp.bfloat16
        sds = jax.ShapeDtypeStruct
        tokens, width = latent.shape
        rows, cols = key_weight.shape
        rank = key_proj.shape[1]
        half = n // 2
        piece = 2 * rank // half
        dma = pltpu.SemaphoreType.DMA
        held = pl.pallas_call(
            functools.partial(exchange_kernel, n, m),
            out_shape=(
                sds((half, piece, cols), bf16),
                sds((n, 2, rows, cols), bf16),
                sds((n, 2, cols), f32),
                sds((2, rows, cols), f32),
                sds((2, width, rank), bf16),
                sds((4, rank, cols), f32),
            ),
            in_specs=[HBM] * 11,
            out_specs=(VMEM,) * 6,
            scratch_shapes=[
                pltpu.VMEM((CHUNKS, tokens, width // CHUNKS), bf16),
                pltpu.VMEM((2, tokens, cols), bf16),
                pltpu.VMEM((2 * cols, tokens), bf16),
                pltpu.VMEM((2 * cols, width), bf16),
                pltpu.VMEM((2 * rank, cols), bf16),
                pltpu.VMEM((2 * rank, cols), bf16),
                pltpu.VMEM((half - 1, piece, cols), bf16),
                pltpu.VMEM((m, 2, cols), f32),
                dma((4,)),
                dma((CHUNKS,)),
                dma,
                dma,
                dma,
                dma,
                dma,
                dma,
                dma,
                dma,
                dma,
                dma((half,)),
                dma,
                dma,
                dma,
                dma,
                dma,
                dma((n,)),
                dma,
                dma,
                dma,
            ],
            compiler_params=pltpu.CompilerParams(
                collective_id=0, has_side_effects=True, vmem_limit_bytes=24 << 20
            ),
        )(
            *(
                pltpu.with_memory_space_constraint(x, pltpu.MemorySpace.HBM)
                for x in (
                    latent,
                    key_cot,
                    value_cot,
                    key_weight,
                    value_weight,
                    key_proj,
                    value_proj,
                    key_first,
                    key_second,
                    value_first,
                    value_second,
                )
            )
        )
        small = sds((rows, cols), f32)
        moment = sds((rank, cols), f32)
        copy = sds((n * rows, cols), bf16)
        return pl.pallas_call(
            functools.partial(update_kernel, n, float(rows * cols * n * m)),
            out_shape=(small,) * 4 + (moment,) * 4 + (copy,) * 2,
            in_specs=[VMEM] * 6,
            out_specs=(HBM,) * 10,
            scratch_shapes=[
                pltpu.VMEM((4, rows, cols), f32),
                pltpu.VMEM((4, rank, cols), f32),
                pltpu.VMEM((2, n * rows, cols), bf16),
                dma((3,)),
            ],
            compiler_params=pltpu.CompilerParams(vmem_limit_bytes=24 << 20),
        )(*held)

    split, column = P("fs", "tp"), P(None, "tp")
    return jax.shard_map(
        body,
        mesh=mesh,
        in_specs=(P("fs", None),) + (split,) * 4 + (P(),) * 2 + (column,) * 4,
        out_specs=(split,) * 4 + (column,) * 6,
        check_vma=False,
    )
```

```python
import functools

import jax
import jax.numpy as jnp
from jax import lax
from jax.experimental import pallas as pl
from jax.experimental.pallas import tpu as pltpu
from jax.sharding import PartitionSpec as P

EPSILON = 1e-08
FIRST_DECAY = 0.7
SECOND_DECAY = 0.8
LEARN_RATE = 0.2
CUTS = (0, 1, 2, 4)
BARRIER_CHUNK = 1
DOT_COLS = 256
MESH = pl.DeviceIdType.MESH
HBM = pl.BlockSpec(memory_space=pltpu.MemorySpace.HBM)
VMEM = pl.BlockSpec(memory_space=pltpu.MemorySpace.VMEM)


def exchange_kernel(
    n,
    m,
    entries,
    latent,
    key_cot,
    value_cot,
    key_weight,
    value_weight,
    key_proj,
    value_proj,
    key_first,
    key_second,
    value_first,
    value_second,
    small,
    moment,
    copied,
    gathered,
    weights,
    weight_v,
    proj_v,
    moment_v,
    latent_v,
    cot_v,
    cot_t,
    reduced,
    partial,
    joined,
    turned,
    steps,
    received,
    own_squares,
    hub_squares,
    tp_squares,
    squares,
    load_sem,
    latent_sem,
    send_sem,
    recv_sem,
    weight_sem,
    square_sem,
):
    me = lax.axis_index("fs")
    mine = lax.axis_index("tp")
    core = lax.rem(me, 2)
    chip = lax.div(me, 2)
    partner = me + 1 - 2 * core
    half = n // 2
    width = latent.shape[1]
    rank = key_proj.shape[1]
    rows, cols = key_weight.shape
    owners, piece = gathered.shape[:2]
    first_owner = (half - owners) // 2
    f32, bf16 = jnp.float32, jnp.bfloat16
    chunks = [
        (a * width // CUTS[-1], (b - a) * width // CUTS[-1])
        for a, b in zip(CUTS, CUTS[1:])
    ]

    def load(src, dst, sem):
        pltpu.make_async_copy(src, dst, sem).start()

    def landed(ref, sem):
        pltpu.make_async_copy(ref, ref, sem).wait()

    load(key_cot, cot_v.at[0], load_sem.at[0])
    load(value_cot, cot_v.at[1], load_sem.at[0])
    for c, (start, size) in enumerate(chunks):
        part = (slice(None), pl.ds(start, size))
        load(latent.at[part], latent_v.at[part], latent_sem.at[c])
        if c == 0:
            load(key_weight, weight_v.at[0], load_sem.at[1])
            load(value_weight, weight_v.at[1], load_sem.at[1])

    barrier = pltpu.get_barrier_semaphore()
    for d in range(1, n):
        pl.semaphore_signal(
            barrier, inc=1, device_id={"fs": lax.rem(me + d, n)}, device_id_type=MESH
        )

    hub = me == 0

    @pl.when(hub)
    def _():
        for d in range(1, m):
            pl.semaphore_signal(
                barrier,
                inc=1,
                device_id={"tp": lax.rem(mine + d, m)},
                device_id_type=MESH,
            )

    def remote(src, dst, sem, arrival, where):
        return pltpu.make_async_remote_copy(
            src_ref=src,
            dst_ref=dst,
            send_sem=sem,
            recv_sem=arrival,
            device_id=where,
            device_id_type=MESH,
        )

    def send(src, dst, arrival, where):
        remote(src, dst, send_sem, arrival, where).start()

    def arrived(ref, sem):
        remote(ref, ref, sem, sem, {"fs": partner}).wait_recv()

    def left(ref, sem):
        remote(ref, ref, sem, sem, {"fs": partner}).wait_send()

    def all_left(elements):
        left(latent_v.at[pl.ds(0, elements // width)], send_sem)

    side = lax.div(chip, (half + 1) // 2)

    def far_first(k):
        down = half - 1 - k
        down = down - lax.div(chip - down + half, half)
        up = k + lax.div(k - chip + half, half)
        return down + side * (up - down)

    def near_first(k):
        return far_first(half - 2 - k)

    def direct(source, target):
        return (
            ((target > 0) & (target < half - 1))
            | (abs(target - source) <= 1)
            | ((target == 0) & (source == 2))
        )

    def late(source, target):
        return (source == 2) & (target == 1)

    def direct_count(c):
        return sum(bool(direct(c, t)) for t in range(half) if t != c)

    def relay_count(c):
        return sum(
            2 * (not direct(t, end))
            for end, near in ((0, 1), (half - 1, half - 2))
            for t in range(half)
            if c == near
        )

    piece_at, weight_at = recv_sem.at[0], recv_sem.at[1]

    def join_at(i):
        return recv_sem.at[3 + owners + i]

    partner_at = recv_sem.at[0]

    def total_at(i):
        return recv_sem.at[1 + i]

    def summed_at(owner):
        return recv_sem.at[3 + owner]

    def owns(c):
        return (c >= first_owner) & (c < first_owner + owners)

    def shard_at(source, i):
        return weight_sem.at[source, i]

    def spread(now_late):
        for i in range(2):
            for k in range(half - 1):
                target = far_first(k)

                @pl.when(direct(chip, target) & (late(chip, target) == now_late))
                def _():
                    send(
                        weights.at[me, i],
                        weights.at[me, i],
                        shard_at(me, i),
                        {"fs": 2 * target},
                    )

    def enter():
        with jax.named_scope("bar"):
            pl.semaphore_wait(barrier, n - 1 + jnp.where(hub, m - 1, 0))

        @pl.when(~hub)
        def _():
            remote(
                own_squares,
                hub_squares.at[me],
                square_sem.at[0],
                square_sem.at[1],
                {"fs": 0},
            ).start()

        spread(False)

        @pl.when(core == 0)
        def _():
            send(weights.at[me], weights.at[me], weight_at, {"fs": partner})

        @pl.when(core == 1)
        def _():
            send(weights.at[me], weights.at[me], partner_at, {"fs": partner})

    with jax.named_scope("cot"):
        landed(cot_v, load_sem.at[0])
    for i in range(2):
        cot_t[pl.ds(i * cols, cols), :] = cot_v[i].T

    for c, (start, size) in enumerate(chunks):
        if c == BARRIER_CHUNK:
            with jax.named_scope("wt"):
                landed(weight_v, load_sem.at[1])
            for i in range(2):
                w = weight_v[i]
                weights[me, i] = w.astype(bf16)
                own_squares[pl.ds(i, 1), :] = jnp.sum(w * w, axis=0, keepdims=True)
            pl.when(chip > 0)(enter)

        part = pl.ds(start, size)
        with jax.named_scope(f"lat{c}"):
            landed(latent_v.at[:, part], latent_sem.at[c])
        if c == 0:
            load(key_proj, proj_v.at[0], load_sem.at[0])
            load(value_proj, proj_v.at[1], load_sem.at[0])
        if c == BARRIER_CHUNK:
            load(key_first, moment_v.at[0], load_sem.at[1])
            load(key_second, moment_v.at[1], load_sem.at[1])
            load(value_first, moment_v.at[2], load_sem.at[1])
            load(value_second, moment_v.at[3], load_sem.at[1])
        for at in range(start, start + size, DOT_COLS):
            for i in range(2):
                head = pl.ds(i * cols, cols)
                reduced[head, pl.ds(at, DOT_COLS)] = jnp.dot(
                    cot_t[head, :],
                    latent_v[:, pl.ds(at, DOT_COLS)],
                    preferred_element_type=f32,
                ).astype(bf16)
    landed(proj_v, load_sem.at[0])
    totals = [
        jnp.dot(
            reduced[pl.ds(i * cols, cols), :], proj_v[i], preferred_element_type=f32
        )
        for i in range(2)
    ]
    pl.when(chip == 0)(enter)

    @pl.when(core == 0)
    def _():
        for i in range(2):
            part = pl.ds(i * rank, rank)
            partial[part, :] = totals[i].astype(bf16).T
            send(partial.at[part], joined.at[part], join_at(i), {"fs": partner})
        shift = jnp.where(chip == 1, 2, jnp.where(chip == half - 2, 1, 0))
        for k in range(half - 1):
            if k == 0:

                @pl.when(hub)
                def _():
                    with jax.named_scope("hub"):
                        arrived(hub_squares.at[pl.ds(1, n - 1)], square_sem.at[1])
                    hub_squares[0] = own_squares[...]
                    tp_squares[mine] = jnp.sum(hub_squares[...], axis=0)
                    for d in range(1, m):
                        remote(
                            tp_squares.at[mine],
                            tp_squares.at[mine],
                            square_sem.at[2],
                            square_sem.at[3],
                            {"tp": lax.rem(mine + d, m)},
                        ).start()

            if k == min(1, half - 2):
                spread(True)

            if k == half - 2:

                @pl.when(hub)
                def _():
                    with jax.named_scope("hubtp"):
                        arrived(tp_squares.at[pl.ds(0, m - 1)], square_sem.at[3])
                    squares[...] = jnp.sum(tp_squares[...], axis=0)
                    for d in range(1, n):
                        remote(
                            squares,
                            squares,
                            square_sem.at[0],
                            square_sem.at[1],
                            {"fs": d},
                        ).start()

            origin = near_first(lax.rem(k + shift, half - 1))
            for i in range(2):
                for part in range(2):
                    source = 2 * origin + part
                    shard = weights.at[source, i]
                    with jax.named_scope(f"w{k}{i}{part}"):
                        arrived(shard, shard_at(source, i))
                    for end, near in ((0, 1), (half - 1, half - 2)):

                        @pl.when((chip == near) & ~direct(origin, end))
                        def _():
                            send(shard, shard, shard_at(source, i), {"fs": 2 * end})

                    send(shard, shard, weight_at, {"fs": partner})
        with jax.named_scope("xw"):
            arrived(weights.at[partner], partner_at)

    @pl.when(core == 1)
    def _():
        for i in range(2):
            turned[i] = totals[i].T
        for i in range(2):
            part = pl.ds(i * rank, rank)
            with jax.named_scope(f"join{i}"):
                arrived(joined.at[part], join_at(i))
            partial[part, :] = (turned[i] + joined[part, :].astype(f32)).astype(bf16)
        for k in range(half - 1):
            target = far_first(lax.rem(k + side, half - 1))

            @pl.when(owns(target))
            def _():
                send(
                    partial.at[pl.ds((target - first_owner) * piece, piece)],
                    received.at[lax.rem(target - chip + half, half) - 1],
                    piece_at,
                    {"fs": 2 * target + 1},
                )

        spread(True)

        @pl.when(owns(chip))
        def _():
            mine_at = chip - first_owner
            with jax.named_scope("rs"):
                arrived(received, piece_at)
            own = partial[pl.ds(pl.multiple_of(mine_at * piece, piece), piece), :]
            gathered[mine_at] = (
                own.astype(f32) + jnp.sum(received[...].astype(f32), axis=0)
            ).astype(bf16)
            for k in range(half - 1):
                send(
                    gathered.at[mine_at],
                    gathered.at[mine_at],
                    summed_at(mine_at),
                    {"fs": 2 * far_first(k) + 1},
                )
            send(
                gathered.at[mine_at],
                gathered.at[mine_at],
                total_at(lax.div(2 * mine_at, owners)),
                {"fs": partner},
            )

        for k in range(half - 1):
            source = near_first(k)

            @pl.when(owns(source))
            def _():
                owner = source - first_owner
                with jax.named_scope(f"ag{k}"):
                    arrived(gathered.at[owner], summed_at(owner))
                send(
                    gathered.at[owner],
                    gathered.at[owner],
                    total_at(lax.div(2 * owner, owners)),
                    {"fs": partner},
                )

    landed(moment_v, load_sem.at[1])

    @pl.when(core == 0)
    def _():
        for i in range(2):
            with jax.named_scope(f"final{i}"):
                arrived(gathered.at[pl.ds(i * owners // 2, owners // 2)], total_at(i))

    both = gathered[...].astype(f32).reshape(2 * rank, cols)
    normalized = []
    for i in range(2):
        projected = both[i * rank : (i + 1) * rank]
        first_new = FIRST_DECAY * moment_v[2 * i] + (1.0 - FIRST_DECAY) * projected
        second_new = (
            SECOND_DECAY * moment_v[2 * i + 1]
            + (1.0 - SECOND_DECAY) * projected * projected
        )
        moment[2 * i] = first_new
        moment[2 * i + 1] = second_new
        normalized.append((first_new / (jnp.sqrt(second_new) + EPSILON)).astype(bf16))

    @pl.when(~hub)
    def _():
        with jax.named_scope("sq"):
            arrived(squares, square_sem.at[1])

    for i in range(2):
        total = jnp.sum(squares[pl.ds(i, 1), :], keepdims=True)
        scale = LEARN_RATE * jnp.sqrt(total / entries)
        steps[i] = scale * jnp.dot(
            proj_v[i], normalized[i], preferred_element_type=f32
        )

    @pl.when(core == 1)
    def _():
        with jax.named_scope("fw"):
            arrived(weights.at[pl.ds(0, n - 1)], weight_at)

    for i in range(2):
        own_step = steps[i, pl.ds(pl.multiple_of(me * rows, rows), rows), :]
        small[2 + i] = own_step
        small[i] = weight_v[i] - own_step
        held = weights[:, i].astype(f32).reshape(n * rows, cols)
        copied[i] = (held - steps[i]).astype(bf16)

    shard_size = 2 * rows * cols
    for c in range(half):
        sent_pieces = 2 * owners
        if first_owner <= c < first_owner + owners:
            sent_pieces += half - 2
        shards = [1 + direct_count(c)] * 2
        shards[0] += n - 2 + relay_count(c)

        @pl.when((chip == c) & (core == 0))
        def _():
            all_left(2 * rank * cols + shards[0] * shard_size)

        @pl.when((chip == c) & (core == 1))
        def _():
            all_left(sent_pieces * piece * cols + shards[1] * shard_size)

    @pl.when(hub)
    def _():
        left(tp_squares.at[pl.ds(0, m - 1)], square_sem.at[2])
        left(hub_squares.at[pl.ds(0, n - 1)], square_sem.at[0])

    @pl.when(~hub)
    def _():
        left(own_squares, square_sem.at[0])


def store_kernel(small, moment, copied, *refs):
    outs, sems = refs[:10], refs[10]
    pairs = [(moment.at[i], outs[4 + i], 0) for i in range(4)]
    pairs += [(copied.at[i], outs[8 + i], 1) for i in range(2)]
    pairs += [(small.at[i], outs[i], 2) for i in range(4)]
    for src, out, sem in pairs:
        pltpu.make_async_copy(src, out, sems.at[sem]).start()
    for sem, ref in enumerate((moment, copied, small)):
        pltpu.make_async_copy(ref, ref, sems.at[sem]).wait()


def solution(mesh):
    n, m = mesh.shape["fs"], mesh.shape["tp"]
    half = n // 2
    owners = half

    def body(latent, key_cot, value_cot, key_weight, value_weight, key_proj, *rest):
        f32, bf16 = jnp.float32, jnp.bfloat16
        sds = jax.ShapeDtypeStruct
        tokens, width = latent.shape
        rows, cols = key_weight.shape
        rank = key_proj.shape[1]
        piece = 2 * rank // owners
        dma = pltpu.SemaphoreType.DMA
        operands = latent, key_cot, value_cot, key_weight, value_weight, key_proj, *rest
        held = pl.pallas_call(
            functools.partial(exchange_kernel, n, m, float(rows * cols * n * m)),
            out_shape=(
                sds((4, rows, cols), f32),
                sds((4, rank, cols), f32),
                sds((2, n * rows, cols), bf16),
            ),
            in_specs=[HBM] * 11,
            out_specs=(VMEM,) * 3,
            scratch_shapes=[
                pltpu.VMEM((owners, piece, cols), bf16),
                pltpu.VMEM((n, 2, rows, cols), bf16),
                pltpu.VMEM((2, rows, cols), f32),
                pltpu.VMEM((2, width, rank), bf16),
                pltpu.VMEM((4, rank, cols), f32),
                pltpu.VMEM((tokens, width), bf16),
                pltpu.VMEM((2, tokens, cols), bf16),
                pltpu.VMEM((2 * cols, tokens), bf16),
                pltpu.VMEM((2 * cols, width), bf16),
                pltpu.VMEM((2 * rank, cols), bf16),
                pltpu.VMEM((2 * rank, cols), bf16),
                pltpu.VMEM((2, rank, cols), f32),
                pltpu.VMEM((2, n * rows, cols), f32),
                pltpu.VMEM((half - 1, piece, cols), bf16),
                pltpu.VMEM((2, cols), f32),
                pltpu.VMEM((n, 2, cols), f32),
                pltpu.VMEM((m, 2, cols), f32),
                pltpu.VMEM((2, cols), f32),
                dma((2,)),
                dma((len(CUTS) - 1,)),
                dma,
                dma((5 + owners,)),
                dma((n, 2)),
                dma((4,)),
            ],
            compiler_params=pltpu.CompilerParams(
                collective_id=0, has_side_effects=True, vmem_limit_bytes=24 << 20
            ),
        )(
            *(
                pltpu.with_memory_space_constraint(x, pltpu.MemorySpace.HBM)
                for x in operands
            )
        )
        return pl.pallas_call(
            store_kernel,
            out_shape=(sds((rows, cols), f32),) * 4
            + (sds((rank, cols), f32),) * 4
            + (sds((n * rows, cols), bf16),) * 2,
            in_specs=[VMEM] * 3,
            out_specs=(HBM,) * 10,
            scratch_shapes=[dma((3,))],
            compiler_params=pltpu.CompilerParams(vmem_limit_bytes=24 << 20),
        )(*held)

    split, column = P("fs", "tp"), P(None, "tp")
    return jax.shard_map(
        body,
        mesh=mesh,
        in_specs=(P("fs", None),) + (split,) * 4 + (P(),) * 2 + (column,) * 4,
        out_specs=(split,) * 4 + (column,) * 6,
        check_vma=False,
    )
```

```python
import functools

import jax
import jax.numpy as jnp
from jax import lax
from jax.experimental import pallas as pl
from jax.experimental.pallas import tpu as pltpu
from jax.sharding import PartitionSpec as P

EPSILON = 1e-08
FIRST_DECAY = 0.7
SECOND_DECAY = 0.8
LEARN_RATE = 0.2
CUTS = (0, 1, 2, 4)
BARRIER_CHUNK = 1
DOT_COLS = 256
MESH = pl.DeviceIdType.MESH
HBM = pl.BlockSpec(memory_space=pltpu.MemorySpace.HBM)
VMEM = pl.BlockSpec(memory_space=pltpu.MemorySpace.VMEM)


def exchange_kernel(
    n,
    m,
    entries,
    latent,
    key_cot,
    value_cot,
    key_weight,
    value_weight,
    key_proj,
    value_proj,
    key_first,
    key_second,
    value_first,
    value_second,
    small,
    moment,
    copied,
    gathered,
    weights,
    weight_v,
    proj_v,
    moment_v,
    latent_v,
    cot_v,
    cot_t,
    reduced,
    partial,
    joined,
    turned,
    steps,
    normalized,
    received,
    own_squares,
    hub_squares,
    tp_squares,
    squares,
    load_sem,
    latent_sem,
    send_sem,
    recv_sem,
    square_sem,
):
    me = lax.axis_index("fs")
    mine = lax.axis_index("tp")
    core = lax.rem(me, 2)
    chip = lax.div(me, 2)
    partner = me + 1 - 2 * core
    half = n // 2
    width = latent.shape[1]
    rank = key_proj.shape[1]
    rows, cols = key_weight.shape
    piece = gathered.shape[1]
    f32, bf16 = jnp.float32, jnp.bfloat16
    chunks = [
        (a * width // CUTS[-1], (b - a) * width // CUTS[-1])
        for a, b in zip(CUTS, CUTS[1:])
    ]

    def load(src, dst, sem):
        pltpu.make_async_copy(src, dst, sem).start()

    def landed(ref, sem):
        pltpu.make_async_copy(ref, ref, sem).wait()

    load(key_cot, cot_v.at[0], load_sem.at[0])
    load(value_cot, cot_v.at[1], load_sem.at[0])
    for c, (start, size) in enumerate(chunks):
        part = (slice(None), pl.ds(start, size))
        load(latent.at[part], latent_v.at[part], latent_sem.at[c])
        if c == 0:
            load(key_weight, weight_v.at[0], load_sem.at[1])
            load(value_weight, weight_v.at[1], load_sem.at[1])

    barrier = pltpu.get_barrier_semaphore()
    for d in range(1, n):
        pl.semaphore_signal(
            barrier, inc=1, device_id={"fs": lax.rem(me + d, n)}, device_id_type=MESH
        )

    hub = me == 0

    @pl.when(hub)
    def _():
        for d in range(1, m):
            pl.semaphore_signal(
                barrier,
                inc=1,
                device_id={"tp": lax.rem(mine + d, m)},
                device_id_type=MESH,
            )

    def remote(src, dst, sem, arrival, where):
        return pltpu.make_async_remote_copy(
            src_ref=src,
            dst_ref=dst,
            send_sem=sem,
            recv_sem=arrival,
            device_id=where,
            device_id_type=MESH,
        )

    def send(src, dst, arrival, where):
        remote(src, dst, send_sem, arrival, where).start()

    def arrived(ref, sem):
        remote(ref, ref, sem, sem, {"fs": partner}).wait_recv()

    def left(ref, sem):
        remote(ref, ref, sem, sem, {"fs": partner}).wait_send()

    def all_left(elements):
        left(latent_v.at[pl.ds(0, elements // width)], send_sem)

    side = lax.div(chip, (half + 1) // 2)

    def far_first(k):
        down = half - 1 - k
        down = down - lax.div(chip - down + half, half)
        up = k + lax.div(k - chip + half, half)
        return down + side * (up - down)

    def near_first(k):
        return far_first(half - 2 - k)

    def direct(source, target):
        return (
            ((target > 0) & (target < half - 1))
            | (abs(target - source) <= 1)
            | ((target == 0) & (source == 2))
        )

    def turn(target):
        last = ((chip == 2) & (target == 1)) | (
            (chip == half - 1) & (target == half - 2)
        )
        return jnp.where(last, 2, jnp.where((core == 1) & (chip == 0), 1, 0))

    def direct_count(c):
        return sum(bool(direct(c, t)) for t in range(half) if t != c)

    def relay_count(c):
        return sum(
            2 * (not direct(t, end))
            for end, near in ((0, 1), (half - 1, half - 2))
            for t in range(half)
            if c == near
        )

    def slot(source, target):
        return lax.rem(source - target + half, half) - 1

    piece_at, weight_at = recv_sem.at[0], recv_sem.at[1]

    def join_at(i):
        return recv_sem.at[2 + i]

    def summed_at(owner, target):
        return recv_sem.at[4 + slot(owner, target)]

    partner_at = recv_sem.at[0]

    def total_at(owner):
        return recv_sem.at[1 + owner]

    def shard_at(source, target, i):
        return recv_sem.at[1 + half + 2 * slot(source, target) + i]

    def spread(now):
        for i in range(2):
            for k in range(half - 1):
                target = far_first(k)

                @pl.when(direct(chip, target) & (turn(target) == now))
                def _():
                    send(
                        weights.at[me, i],
                        weights.at[me, i],
                        shard_at(chip, target, i),
                        {"fs": 2 * target},
                    )

    def enter():
        with jax.named_scope("bar"):
            pl.semaphore_wait(barrier, n - 1 + jnp.where(hub, m - 1, 0))

        @pl.when(~hub)
        def _():
            remote(
                own_squares,
                hub_squares.at[me],
                square_sem.at[0],
                square_sem.at[1],
                {"fs": 0},
            ).start()

        spread(0)

        @pl.when(core == 0)
        def _():
            send(weights.at[me], weights.at[me], weight_at, {"fs": partner})

        @pl.when(core == 1)
        def _():
            send(weights.at[me], weights.at[me], partner_at, {"fs": partner})

    with jax.named_scope("cot"):
        landed(cot_v, load_sem.at[0])
    for i in range(2):
        cot_t[pl.ds(i * cols, cols), :] = cot_v[i].T

    for c, (start, size) in enumerate(chunks):
        if c == BARRIER_CHUNK:
            with jax.named_scope("wt"):
                landed(weight_v, load_sem.at[1])
            for i in range(2):
                w = weight_v[i]
                weights[me, i] = w.astype(bf16)
                own_squares[pl.ds(i, 1), :] = jnp.sum(w * w, axis=0, keepdims=True)
            pl.when(chip > 0)(enter)

        part = pl.ds(start, size)
        with jax.named_scope(f"lat{c}"):
            landed(latent_v.at[:, part], latent_sem.at[c])
        if c == 0:
            load(key_proj, proj_v.at[0], load_sem.at[0])
            load(value_proj, proj_v.at[1], load_sem.at[0])
        if c == BARRIER_CHUNK:
            load(key_first, moment_v.at[0], load_sem.at[1])
            load(key_second, moment_v.at[1], load_sem.at[1])
            load(value_first, moment_v.at[2], load_sem.at[1])
            load(value_second, moment_v.at[3], load_sem.at[1])
        for at in range(start, start + size, DOT_COLS):
            for i in range(2):
                head = pl.ds(i * cols, cols)
                reduced[head, pl.ds(at, DOT_COLS)] = jnp.dot(
                    cot_t[head, :],
                    latent_v[:, pl.ds(at, DOT_COLS)],
                    preferred_element_type=f32,
                ).astype(bf16)
    landed(proj_v, load_sem.at[0])
    totals = [
        jnp.dot(
            reduced[pl.ds(i * cols, cols), :], proj_v[i], preferred_element_type=f32
        )
        for i in range(2)
    ]
    pl.when(chip == 0)(enter)

    @pl.when(core == 0)
    def _():
        for i in range(2):
            part = pl.ds(i * rank, rank)
            partial[part, :] = totals[i].astype(bf16).T
            send(partial.at[part], joined.at[part], join_at(i), {"fs": partner})
        shift = jnp.where(chip == 1, 2, jnp.where(chip == half - 2, 1, 0))
        for k in range(half - 1):
            if k == 0:

                @pl.when(hub)
                def _():
                    with jax.named_scope("hub"):
                        arrived(hub_squares.at[pl.ds(1, n - 1)], square_sem.at[1])
                    hub_squares[0] = own_squares[...]
                    tp_squares[mine] = jnp.sum(hub_squares[...], axis=0)
                    for d in range(1, m):
                        remote(
                            tp_squares.at[mine],
                            tp_squares.at[mine],
                            square_sem.at[2],
                            square_sem.at[3],
                            {"tp": lax.rem(mine + d, m)},
                        ).start()

            if k == min(1, half - 2):
                spread(2)

            if k == half - 2:

                @pl.when(hub)
                def _():
                    with jax.named_scope("hubtp"):
                        arrived(tp_squares.at[pl.ds(0, m - 1)], square_sem.at[3])
                    squares[...] = jnp.sum(tp_squares[...], axis=0)
                    for d in range(1, n):
                        remote(
                            squares,
                            squares,
                            square_sem.at[0],
                            square_sem.at[1],
                            {"fs": d},
                        ).start()

            origin = near_first(lax.rem(k + shift, half - 1))
            for i in range(2):
                shards = weights.at[pl.ds(2 * origin, 2), i]
                with jax.named_scope(f"w{k}{i}"):
                    arrived(shards, shard_at(origin, chip, i))
                for end, near in ((0, 1), (half - 1, half - 2)):

                    @pl.when((chip == near) & ~direct(origin, end))
                    def _():
                        send(
                            shards, shards, shard_at(origin, end, i), {"fs": 2 * end}
                        )

                send(shards, shards, weight_at, {"fs": partner})
        with jax.named_scope("xw"):
            arrived(weights.at[partner], partner_at)

    @pl.when(core == 1)
    def _():
        for i in range(2):
            turned[i] = totals[i].T
        for i in range(2):
            part = pl.ds(i * rank, rank)
            with jax.named_scope(f"join{i}"):
                arrived(joined.at[part], join_at(i))
            partial[part, :] = (turned[i] + joined[part, :].astype(f32)).astype(bf16)
        for k in range(half - 1):
            target = far_first(lax.rem(k + side, half - 1))
            send(
                partial.at[pl.ds(target * piece, piece)],
                received.at[slot(chip, target)],
                piece_at,
                {"fs": 2 * target + 1},
            )
        spread(1)
        with jax.named_scope("rs"):
            arrived(received, piece_at)
        own = partial[pl.ds(pl.multiple_of(chip * piece, piece), piece), :]
        gathered[chip] = (
            own.astype(f32) + jnp.sum(received[...].astype(f32), axis=0)
        ).astype(bf16)
        for k in range(half - 1):
            target = far_first(k)
            send(
                gathered.at[chip],
                gathered.at[chip],
                summed_at(chip, target),
                {"fs": 2 * target + 1},
            )
        send(gathered.at[chip], gathered.at[chip], total_at(chip), {"fs": partner})
        spread(2)
        for k in range(half - 1):
            owner = near_first(k)
            with jax.named_scope(f"ag{k}"):
                arrived(gathered.at[owner], summed_at(owner, chip))
            send(
                gathered.at[owner], gathered.at[owner], total_at(owner), {"fs": partner}
            )

    landed(moment_v, load_sem.at[1])

    for owner in range(half):

        @pl.when(core == 0)
        def _():
            with jax.named_scope(f"final{owner}"):
                arrived(gathered.at[owner], total_at(owner))

        i, start = divmod(owner * piece, rank)
        part = pl.ds(start, piece)
        projected = gathered[owner].astype(f32)
        first_new = (
            FIRST_DECAY * moment_v[2 * i, part, :] + (1.0 - FIRST_DECAY) * projected
        )
        second_new = (
            SECOND_DECAY * moment_v[2 * i + 1, part, :]
            + (1.0 - SECOND_DECAY) * projected * projected
        )
        moment[2 * i, part, :] = first_new
        moment[2 * i + 1, part, :] = second_new
        normalized[i, part, :] = (
            first_new / (jnp.sqrt(second_new) + EPSILON)
        ).astype(bf16)
        if start + piece < rank:
            continue
        if i == 0:

            @pl.when(~hub)
            def _():
                with jax.named_scope("sq"):
                    arrived(squares, square_sem.at[1])

        total = jnp.sum(squares[pl.ds(i, 1), :], keepdims=True)
        scale = LEARN_RATE * jnp.sqrt(total / entries)
        for at in range(0, width, width // 2):
            some = pl.ds(at, width // 2)
            steps[i, some, :] = scale * jnp.dot(
                proj_v[i, some, :], normalized[i], preferred_element_type=f32
            )

    @pl.when(core == 1)
    def _():
        with jax.named_scope("fw"):
            arrived(weights.at[pl.ds(0, n - 1)], weight_at)

    for i in range(2):
        own_step = steps[i, pl.ds(pl.multiple_of(me * rows, rows), rows), :]
        small[2 + i] = own_step
        small[i] = weight_v[i] - own_step
        held = weights[:, i].astype(f32).reshape(n * rows, cols)
        copied[i] = (held - steps[i]).astype(bf16)

    shard_size = 2 * rows * cols
    for c in range(half):
        sent_pieces = 3 * half - 2
        shards = [1 + direct_count(c)] * 2
        shards[0] += n - 2 + relay_count(c)

        @pl.when((chip == c) & (core == 0))
        def _():
            all_left(2 * rank * cols + shards[0] * shard_size)

        @pl.when((chip == c) & (core == 1))
        def _():
            all_left(sent_pieces * piece * cols + shards[1] * shard_size)

    @pl.when(hub)
    def _():
        left(tp_squares.at[pl.ds(0, m - 1)], square_sem.at[2])
        left(hub_squares.at[pl.ds(0, n - 1)], square_sem.at[0])

    @pl.when(~hub)
    def _():
        left(own_squares, square_sem.at[0])


def store_kernel(small, moment, copied, *refs):
    outs, sems = refs[:10], refs[10]
    pairs = [(moment.at[i], outs[4 + i], 0) for i in range(4)]
    pairs += [(copied.at[i], outs[8 + i], 1) for i in range(2)]
    pairs += [(small.at[i], outs[i], 2) for i in range(4)]
    for src, out, sem in pairs:
        pltpu.make_async_copy(src, out, sems.at[sem]).start()
    for sem, ref in enumerate((moment, copied, small)):
        pltpu.make_async_copy(ref, ref, sems.at[sem]).wait()


def solution(mesh):
    n, m = mesh.shape["fs"], mesh.shape["tp"]
    half = n // 2

    def body(latent, key_cot, value_cot, key_weight, value_weight, key_proj, *rest):
        f32, bf16 = jnp.float32, jnp.bfloat16
        sds = jax.ShapeDtypeStruct
        tokens, width = latent.shape
        rows, cols = key_weight.shape
        rank = key_proj.shape[1]
        piece = 2 * rank // half
        dma = pltpu.SemaphoreType.DMA
        operands = latent, key_cot, value_cot, key_weight, value_weight, key_proj, *rest
        held = pl.pallas_call(
            functools.partial(exchange_kernel, n, m, float(rows * cols * n * m)),
            out_shape=(
                sds((4, rows, cols), f32),
                sds((4, rank, cols), f32),
                sds((2, n * rows, cols), bf16),
            ),
            in_specs=[HBM] * 11,
            out_specs=(VMEM,) * 3,
            scratch_shapes=[
                pltpu.VMEM((half, piece, cols), bf16),
                pltpu.VMEM((n, 2, rows, cols), bf16),
                pltpu.VMEM((2, rows, cols), f32),
                pltpu.VMEM((2, width, rank), bf16),
                pltpu.VMEM((4, rank, cols), f32),
                pltpu.VMEM((tokens, width), bf16),
                pltpu.VMEM((2, tokens, cols), bf16),
                pltpu.VMEM((2 * cols, tokens), bf16),
                pltpu.VMEM((2 * cols, width), bf16),
                pltpu.VMEM((2 * rank, cols), bf16),
                pltpu.VMEM((2 * rank, cols), bf16),
                pltpu.VMEM((2, rank, cols), f32),
                pltpu.VMEM((2, n * rows, cols), f32),
                pltpu.VMEM((2, rank, cols), bf16),
                pltpu.VMEM((half - 1, piece, cols), bf16),
                pltpu.VMEM((2, cols), f32),
                pltpu.VMEM((n, 2, cols), f32),
                pltpu.VMEM((m, 2, cols), f32),
                pltpu.VMEM((2, cols), f32),
                dma((2,)),
                dma((len(CUTS) - 1,)),
                dma,
                dma((3 * half - 1,)),
                dma((4,)),
            ],
            compiler_params=pltpu.CompilerParams(
                collective_id=0, has_side_effects=True, vmem_limit_bytes=24 << 20
            ),
        )(
            *(
                pltpu.with_memory_space_constraint(x, pltpu.MemorySpace.HBM)
                for x in operands
            )
        )
        return pl.pallas_call(
            store_kernel,
            out_shape=(sds((rows, cols), f32),) * 4
            + (sds((rank, cols), f32),) * 4
            + (sds((n * rows, cols), bf16),) * 2,
            in_specs=[VMEM] * 3,
            out_specs=(HBM,) * 10,
            scratch_shapes=[dma((3,))],
            compiler_params=pltpu.CompilerParams(vmem_limit_bytes=24 << 20),
        )(*held)

    split, column = P("fs", "tp"), P(None, "tp")
    return jax.shard_map(
        body,
        mesh=mesh,
        in_specs=(P("fs", None),) + (split,) * 4 + (P(),) * 2 + (column,) * 4,
        out_specs=(split,) * 4 + (column,) * 6,
        check_vma=False,
    )
```

```python
import functools

import jax
import jax.numpy as jnp
from jax import lax
from jax.experimental import pallas as pl
from jax.experimental.pallas import tpu as pltpu
from jax.sharding import PartitionSpec as P

EPSILON = 1e-08
FIRST_DECAY = 0.7
SECOND_DECAY = 0.8
LEARN_RATE = 0.2
CUTS = (0, 1, 2, 4)
BARRIER_CHUNK = 1
DOT_COLS = 256
MESH = pl.DeviceIdType.MESH
HBM = pl.BlockSpec(memory_space=pltpu.MemorySpace.HBM)
VMEM = pl.BlockSpec(memory_space=pltpu.MemorySpace.VMEM)


def exchange_kernel(
    n,
    m,
    entries,
    latent,
    key_cot,
    value_cot,
    key_weight,
    value_weight,
    key_proj,
    value_proj,
    key_first,
    key_second,
    value_first,
    value_second,
    small,
    moment,
    copied,
    gathered,
    weights,
    weight_v,
    proj_v,
    moment_v,
    latent_v,
    cot_v,
    cot_t,
    reduced,
    partial,
    joined,
    turned,
    steps,
    normalized,
    received,
    own_squares,
    hub_squares,
    tp_squares,
    squares,
    load_sem,
    latent_sem,
    send_sem,
    recv_sem,
    square_sem,
):
    me = lax.axis_index("fs")
    mine = lax.axis_index("tp")
    core = lax.rem(me, 2)
    chip = lax.div(me, 2)
    partner = me + 1 - 2 * core
    half = n // 2
    width = latent.shape[1]
    rank = key_proj.shape[1]
    rows, cols = key_weight.shape
    piece = gathered.shape[1]
    f32, bf16 = jnp.float32, jnp.bfloat16
    chunks = [
        (a * width // CUTS[-1], (b - a) * width // CUTS[-1])
        for a, b in zip(CUTS, CUTS[1:])
    ]

    def load(src, dst, sem):
        pltpu.make_async_copy(src, dst, sem).start()

    def landed(ref, sem):
        pltpu.make_async_copy(ref, ref, sem).wait()

    load(key_cot, cot_v.at[0], load_sem.at[0])
    load(value_cot, cot_v.at[1], load_sem.at[0])
    for c, (start, size) in enumerate(chunks):
        part = (slice(None), pl.ds(start, size))
        load(latent.at[part], latent_v.at[part], latent_sem.at[c])
        if c == 0:
            load(key_weight, weight_v.at[0], load_sem.at[1])
            load(value_weight, weight_v.at[1], load_sem.at[1])

    barrier = pltpu.get_barrier_semaphore()
    for d in range(1, n):
        pl.semaphore_signal(
            barrier, inc=1, device_id={"fs": lax.rem(me + d, n)}, device_id_type=MESH
        )

    hub = me == 0

    @pl.when(hub)
    def _():
        for d in range(1, m):
            pl.semaphore_signal(
                barrier,
                inc=1,
                device_id={"tp": lax.rem(mine + d, m)},
                device_id_type=MESH,
            )

    def remote(src, dst, sem, arrival, where):
        return pltpu.make_async_remote_copy(
            src_ref=src,
            dst_ref=dst,
            send_sem=sem,
            recv_sem=arrival,
            device_id=where,
            device_id_type=MESH,
        )

    def send(src, dst, arrival, where):
        remote(src, dst, send_sem, arrival, where).start()

    def arrived(ref, sem):
        remote(ref, ref, sem, sem, {"fs": partner}).wait_recv()

    def left(ref, sem):
        remote(ref, ref, sem, sem, {"fs": partner}).wait_send()

    def all_left(elements):
        across = next(
            w
            for w in (width, width // 2, width // 4, width // 8)
            if elements % (16 * w) == 0 and elements <= w * latent_v.shape[0]
        )
        left(latent_v.at[pl.ds(0, elements // across), pl.ds(0, across)], send_sem)

    side = lax.div(chip, (half + 1) // 2)

    def far_first(k):
        down = half - 1 - k
        down = down - lax.div(chip - down + half, half)
        up = k + lax.div(k - chip + half, half)
        return down + side * (up - down)

    def near_first(k):
        return far_first(half - 2 - k)

    def direct(source, target):
        return (
            ((target > 0) & (target < half - 1))
            | (abs(target - source) <= 1)
            | ((target == 0) & (source == 2))
        )

    def turn(target):
        last = ((chip == 2) & (target == 1)) | (
            (chip == half - 1) & (target == half - 2)
        )
        return jnp.where(last, 2, jnp.where((core == 1) & (chip == 0), 1, 0))

    def direct_count(c):
        return sum(bool(direct(c, t)) for t in range(half) if t != c)

    def relay_count(c):
        return sum(
            2 * (not direct(t, end))
            for end, near in ((0, 1), (half - 1, half - 2))
            for t in range(half)
            if c == near
        )

    def slot(source, target):
        return lax.rem(source - target + half, half) - 1

    piece_at, weight_at = recv_sem.at[0], recv_sem.at[1]

    def join_at(i):
        return recv_sem.at[2 + i]

    def summed_at(owner, target):
        return recv_sem.at[4 + slot(owner, target)]

    partner_at = recv_sem.at[0]

    def total_at(owner):
        return recv_sem.at[1 + owner]

    def shard_at(source, target, i):
        return recv_sem.at[1 + half + 2 * slot(source, target) + i]

    def spread(now):
        for i in range(2):
            for k in range(half - 1):
                target = far_first(k)

                @pl.when(direct(chip, target) & (turn(target) == now))
                def _():
                    send(
                        weights.at[me, i],
                        weights.at[me, i],
                        shard_at(chip, target, i),
                        {"fs": 2 * target},
                    )

    def enter():
        with jax.named_scope("bar"):
            pl.semaphore_wait(barrier, n - 1 + jnp.where(hub, m - 1, 0))

        @pl.when(~hub)
        def _():
            remote(
                own_squares,
                hub_squares.at[me],
                square_sem.at[0],
                square_sem.at[1],
                {"fs": 0},
            ).start()

        spread(0)

        @pl.when(core == 0)
        def _():
            send(weights.at[me], weights.at[me], weight_at, {"fs": partner})

        @pl.when(core == 1)
        def _():
            send(weights.at[me], weights.at[me], partner_at, {"fs": partner})

    with jax.named_scope("cot"):
        landed(cot_v, load_sem.at[0])
    for i in range(2):
        cot_t[pl.ds(i * cols, cols), :] = cot_v[i].T

    for c, (start, size) in enumerate(chunks):
        if c == BARRIER_CHUNK:
            with jax.named_scope("wt"):
                landed(weight_v, load_sem.at[1])
            for i in range(2):
                w = weight_v[i]
                weights[me, i] = w.astype(bf16)
                own_squares[pl.ds(i, 1), :] = jnp.sum(w * w, axis=0, keepdims=True)
            pl.when(chip > 1)(enter)
        if c == BARRIER_CHUNK + 1:
            pl.when(chip == 1)(enter)

        part = pl.ds(start, size)
        with jax.named_scope(f"lat{c}"):
            landed(latent_v.at[:, part], latent_sem.at[c])
        if c == 0:
            load(key_proj, proj_v.at[0], load_sem.at[0])
            load(value_proj, proj_v.at[1], load_sem.at[0])
        if c == BARRIER_CHUNK:
            load(key_first, moment_v.at[0], load_sem.at[1])
            load(key_second, moment_v.at[1], load_sem.at[1])
            load(value_first, moment_v.at[2], load_sem.at[1])
            load(value_second, moment_v.at[3], load_sem.at[1])
        for at in range(start, start + size, DOT_COLS):
            for i in range(2):
                head = pl.ds(i * cols, cols)
                reduced[head, pl.ds(at, DOT_COLS)] = jnp.dot(
                    cot_t[head, :],
                    latent_v[:, pl.ds(at, DOT_COLS)],
                    preferred_element_type=f32,
                ).astype(bf16)
    landed(proj_v, load_sem.at[0])
    totals = [
        jnp.dot(
            reduced[pl.ds(i * cols, cols), :], proj_v[i], preferred_element_type=f32
        )
        for i in range(2)
    ]
    pl.when(chip == 0)(enter)

    @pl.when(core == 0)
    def _():
        for i in range(2):
            part = pl.ds(i * rank, rank)
            partial[part, :] = totals[i].astype(bf16).T
            send(partial.at[part], joined.at[part], join_at(i), {"fs": partner})
        shift = jnp.where(chip == 1, 2, jnp.where(chip == half - 2, 1, 0))
        for k in range(half - 1):
            if k == 0:

                @pl.when(hub)
                def _():
                    with jax.named_scope("hub"):
                        arrived(hub_squares.at[pl.ds(1, n - 1)], square_sem.at[1])
                    hub_squares[0] = own_squares[...]
                    tp_squares[mine] = jnp.sum(hub_squares[...], axis=0)
                    for d in range(1, m):
                        remote(
                            tp_squares.at[mine],
                            tp_squares.at[mine],
                            square_sem.at[2],
                            square_sem.at[3],
                            {"tp": lax.rem(mine + d, m)},
                        ).start()

            if k == min(1, half - 2):
                spread(2)

            if k == half - 2:

                @pl.when(hub)
                def _():
                    with jax.named_scope("hubtp"):
                        arrived(tp_squares.at[pl.ds(0, m - 1)], square_sem.at[3])
                    squares[...] = jnp.sum(tp_squares[...], axis=0)
                    for d in range(1, n):
                        remote(
                            squares,
                            squares,
                            square_sem.at[0],
                            square_sem.at[1],
                            {"fs": d},
                        ).start()

            origin = near_first(lax.rem(k + shift, half - 1))
            for i in range(2):
                shards = weights.at[pl.ds(2 * origin, 2), i]
                with jax.named_scope(f"w{k}{i}"):
                    arrived(shards, shard_at(origin, chip, i))
                for end, near in ((0, 1), (half - 1, half - 2)):

                    @pl.when((chip == near) & ~direct(origin, end))
                    def _():
                        send(
                            shards, shards, shard_at(origin, end, i), {"fs": 2 * end}
                        )

                send(shards, shards, weight_at, {"fs": partner})
        with jax.named_scope("xw"):
            arrived(weights.at[partner], partner_at)

    @pl.when(core == 1)
    def _():
        for i in range(2):
            turned[i] = totals[i].T
        for i in range(2):
            part = pl.ds(i * rank, rank)
            with jax.named_scope(f"join{i}"):
                arrived(joined.at[part], join_at(i))
            partial[part, :] = (turned[i] + joined[part, :].astype(f32)).astype(bf16)
        for k in range(half - 1):
            target = far_first(lax.rem(k + side, half - 1))
            send(
                partial.at[pl.ds(target * piece, piece)],
                received.at[slot(chip, target)],
                piece_at,
                {"fs": 2 * target + 1},
            )
        spread(1)
        with jax.named_scope("rs"):
            arrived(received, piece_at)
        own = partial[pl.ds(pl.multiple_of(chip * piece, piece), piece), :]
        gathered[chip] = (
            own.astype(f32) + jnp.sum(received[...].astype(f32), axis=0)
        ).astype(bf16)
        if half > 2:

            @pl.when(chip == 2)
            def _():
                send(gathered.at[chip], gathered.at[chip], total_at(chip), {"fs": 0})

        for k in range(half - 1):
            target = far_first(jnp.where(chip == 0, half - 2 - k, k))
            send(
                gathered.at[chip],
                gathered.at[chip],
                summed_at(chip, target),
                {"fs": 2 * target + 1},
            )
        send(gathered.at[chip], gathered.at[chip], total_at(chip), {"fs": partner})
        spread(2)
        for k in range(half - 1):
            at_zero = 0 if k == 0 else half - 1 - k
            at_one = (k + 1) % (half - 1)
            place = jnp.where(chip == 0, at_zero, jnp.where(chip == 1, at_one, k))
            owner = near_first(place)

            def take(owner=owner, k=k):
                with jax.named_scope(f"ag{k}"):
                    arrived(gathered.at[owner], summed_at(owner, chip))

            if k == half - 2 and half > 2:
                pl.when(chip > 0)(take)
            else:
                take()

            @pl.when((chip > 0) | (owner != 2))
            def _():
                send(
                    gathered.at[owner],
                    gathered.at[owner],
                    total_at(owner),
                    {"fs": partner},
                )

    landed(moment_v, load_sem.at[1])

    def finish(i):
        own_step = steps[i, pl.ds(pl.multiple_of(me * rows, rows), rows), :]
        small[2 + i] = own_step
        small[i] = weight_v[i] - own_step
        held = weights[:, i].astype(f32).reshape(n * rows, cols)
        copied[i] = (held - steps[i]).astype(bf16)

    for owner in range(half):

        @pl.when(core == 0)
        def _():
            with jax.named_scope(f"final{owner}"):
                arrived(gathered.at[owner], total_at(owner))

        if owner == 2:

            @pl.when((core == 1) & (chip == 0))
            def _():
                with jax.named_scope("aglast"):
                    arrived(gathered.at[2], summed_at(2, 0))

        i, start = divmod(owner * piece, rank)
        part = pl.ds(start, piece)
        projected = gathered[owner].astype(f32)
        first_new = (
            FIRST_DECAY * moment_v[2 * i, part, :] + (1.0 - FIRST_DECAY) * projected
        )
        second_new = (
            SECOND_DECAY * moment_v[2 * i + 1, part, :]
            + (1.0 - SECOND_DECAY) * projected * projected
        )
        moment[2 * i, part, :] = first_new
        moment[2 * i + 1, part, :] = second_new
        normalized[i, part, :] = (
            first_new / (jnp.sqrt(second_new) + EPSILON)
        ).astype(bf16)
        if start + piece < rank:
            continue
        if i == 0:

            @pl.when(~hub)
            def _():
                with jax.named_scope("sq"):
                    arrived(squares, square_sem.at[1])

        total = jnp.sum(squares[pl.ds(i, 1), :], keepdims=True)
        scale = LEARN_RATE * jnp.sqrt(total / entries)
        for at in range(0, width, width // 2):
            some = pl.ds(at, width // 2)
            steps[i, some, :] = scale * jnp.dot(
                proj_v[i, some, :], normalized[i], preferred_element_type=f32
            )

        pl.when(core == 0)(lambda: finish(i))

    @pl.when(core == 1)
    def _():
        with jax.named_scope("fw"):
            arrived(weights.at[pl.ds(0, n - 1)], weight_at)
        for i in range(2):
            finish(i)

    shard_size = 2 * rows * cols
    for c in range(half):
        sent_pieces = 3 * half - 2
        if half > 2:
            sent_pieces += (c == 2) - (c == 0)
        shards = [1 + direct_count(c)] * 2
        shards[0] += n - 2 + relay_count(c)

        @pl.when((chip == c) & (core == 0))
        def _():
            all_left(2 * rank * cols + shards[0] * shard_size)

        @pl.when((chip == c) & (core == 1))
        def _():
            all_left(sent_pieces * piece * cols + shards[1] * shard_size)

    @pl.when(hub)
    def _():
        left(tp_squares.at[pl.ds(0, m - 1)], square_sem.at[2])
        left(hub_squares.at[pl.ds(0, n - 1)], square_sem.at[0])

    @pl.when(~hub)
    def _():
        left(own_squares, square_sem.at[0])


def store_kernel(small, moment, copied, *refs):
    outs, sems = refs[:10], refs[10]
    pairs = [(moment.at[i], outs[4 + i], 0) for i in range(4)]
    pairs += [(copied.at[i], outs[8 + i], 1) for i in range(2)]
    pairs += [(small.at[i], outs[i], 2) for i in range(4)]
    for src, out, sem in pairs:
        pltpu.make_async_copy(src, out, sems.at[sem]).start()
    for sem, ref in enumerate((moment, copied, small)):
        pltpu.make_async_copy(ref, ref, sems.at[sem]).wait()


def solution(mesh):
    n, m = mesh.shape["fs"], mesh.shape["tp"]
    half = n // 2

    def body(latent, key_cot, value_cot, key_weight, value_weight, key_proj, *rest):
        f32, bf16 = jnp.float32, jnp.bfloat16
        sds = jax.ShapeDtypeStruct
        tokens, width = latent.shape
        rows, cols = key_weight.shape
        rank = key_proj.shape[1]
        piece = 2 * rank // half
        dma = pltpu.SemaphoreType.DMA
        operands = latent, key_cot, value_cot, key_weight, value_weight, key_proj, *rest
        held = pl.pallas_call(
            functools.partial(exchange_kernel, n, m, float(rows * cols * n * m)),
            out_shape=(
                sds((4, rows, cols), f32),
                sds((4, rank, cols), f32),
                sds((2, n * rows, cols), bf16),
            ),
            in_specs=[HBM] * 11,
            out_specs=(VMEM,) * 3,
            scratch_shapes=[
                pltpu.VMEM((half, piece, cols), bf16),
                pltpu.VMEM((n, 2, rows, cols), bf16),
                pltpu.VMEM((2, rows, cols), f32),
                pltpu.VMEM((2, width, rank), bf16),
                pltpu.VMEM((4, rank, cols), f32),
                pltpu.VMEM((tokens, width), bf16),
                pltpu.VMEM((2, tokens, cols), bf16),
                pltpu.VMEM((2 * cols, tokens), bf16),
                pltpu.VMEM((2 * cols, width), bf16),
                pltpu.VMEM((2 * rank, cols), bf16),
                pltpu.VMEM((2 * rank, cols), bf16),
                pltpu.VMEM((2, rank, cols), f32),
                pltpu.VMEM((2, n * rows, cols), f32),
                pltpu.VMEM((2, rank, cols), bf16),
                pltpu.VMEM((half - 1, piece, cols), bf16),
                pltpu.VMEM((2, cols), f32),
                pltpu.VMEM((n, 2, cols), f32),
                pltpu.VMEM((m, 2, cols), f32),
                pltpu.VMEM((2, cols), f32),
                dma((2,)),
                dma((len(CUTS) - 1,)),
                dma,
                dma((3 * half - 1,)),
                dma((4,)),
            ],
            compiler_params=pltpu.CompilerParams(
                collective_id=0, has_side_effects=True, vmem_limit_bytes=24 << 20
            ),
        )(
            *(
                pltpu.with_memory_space_constraint(x, pltpu.MemorySpace.HBM)
                for x in operands
            )
        )
        return pl.pallas_call(
            store_kernel,
            out_shape=(sds((rows, cols), f32),) * 4
            + (sds((rank, cols), f32),) * 4
            + (sds((n * rows, cols), bf16),) * 2,
            in_specs=[VMEM] * 3,
            out_specs=(HBM,) * 10,
            scratch_shapes=[dma((3,))],
            compiler_params=pltpu.CompilerParams(vmem_limit_bytes=24 << 20),
        )(*held)

    split, column = P("fs", "tp"), P(None, "tp")
    return jax.shard_map(
        body,
        mesh=mesh,
        in_specs=(P("fs", None),) + (split,) * 4 + (P(),) * 2 + (column,) * 4,
        out_specs=(split,) * 4 + (column,) * 6,
        check_vma=False,
    )
```

```python
import functools

import jax
import jax.numpy as jnp
from jax import lax
from jax.experimental import pallas as pl
from jax.experimental.pallas import tpu as pltpu
from jax.sharding import PartitionSpec as P

EPSILON = 1e-08
FIRST_DECAY = 0.7
SECOND_DECAY = 0.8
LEARN_RATE = 0.2
CUTS = (0, 1, 2, 4)
BARRIER_CHUNK = 1
DOT_COLS = 256
MESH = pl.DeviceIdType.MESH
HBM = pl.BlockSpec(memory_space=pltpu.MemorySpace.HBM)
VMEM = pl.BlockSpec(memory_space=pltpu.MemorySpace.VMEM)


def exchange_kernel(
    n,
    m,
    entries,
    latent,
    key_cot,
    value_cot,
    key_weight,
    value_weight,
    key_proj,
    value_proj,
    key_first,
    key_second,
    value_first,
    value_second,
    small,
    moment,
    copied,
    gathered,
    weights,
    weight_v,
    proj_v,
    moment_v,
    latent_v,
    cot_v,
    cot_t,
    reduced,
    partial,
    joined,
    turned,
    steps,
    normalized,
    received,
    own_squares,
    hub_squares,
    tp_squares,
    squares,
    scales,
    load_sem,
    latent_sem,
    send_sem,
    recv_sem,
    square_sem,
):
    me = lax.axis_index("fs")
    mine = lax.axis_index("tp")
    core = lax.rem(me, 2)
    chip = lax.div(me, 2)
    partner = me + 1 - 2 * core
    half = n // 2
    width = latent.shape[1]
    rank = key_proj.shape[1]
    rows, cols = key_weight.shape
    piece = gathered.shape[1]
    f32, bf16 = jnp.float32, jnp.bfloat16
    chunks = [
        (a * width // CUTS[-1], (b - a) * width // CUTS[-1])
        for a, b in zip(CUTS, CUTS[1:])
    ]

    def load(src, dst, sem):
        pltpu.make_async_copy(src, dst, sem).start()

    def landed(ref, sem):
        pltpu.make_async_copy(ref, ref, sem).wait()

    load(key_cot, cot_v.at[0], load_sem.at[0])
    load(value_cot, cot_v.at[1], load_sem.at[0])
    for c, (start, size) in enumerate(chunks):
        part = (slice(None), pl.ds(start, size))
        load(latent.at[part], latent_v.at[part], latent_sem.at[c])
        if c == 0:
            load(key_weight, weight_v.at[0], load_sem.at[1])
            load(value_weight, weight_v.at[1], load_sem.at[1])

    barrier = pltpu.get_barrier_semaphore()
    for d in range(1, n):
        pl.semaphore_signal(
            barrier, inc=1, device_id={"fs": lax.rem(me + d, n)}, device_id_type=MESH
        )

    hub = me == 0

    @pl.when(hub)
    def _():
        for d in range(1, m):
            pl.semaphore_signal(
                barrier,
                inc=1,
                device_id={"tp": lax.rem(mine + d, m)},
                device_id_type=MESH,
            )

    def remote(src, dst, sem, arrival, where):
        return pltpu.make_async_remote_copy(
            src_ref=src,
            dst_ref=dst,
            send_sem=sem,
            recv_sem=arrival,
            device_id=where,
            device_id_type=MESH,
        )

    def send(src, dst, arrival, where):
        remote(src, dst, send_sem, arrival, where).start()

    def arrived(ref, sem):
        remote(ref, ref, sem, sem, {"fs": partner}).wait_recv()

    def left(ref, sem):
        remote(ref, ref, sem, sem, {"fs": partner}).wait_send()

    def all_left(elements):
        across = next(
            w
            for w in (width, width // 2, width // 4, width // 8)
            if elements % (16 * w) == 0 and elements <= w * latent_v.shape[0]
        )
        left(latent_v.at[pl.ds(0, elements // across), pl.ds(0, across)], send_sem)

    side = lax.div(chip, (half + 1) // 2)

    def far_first(k):
        down = half - 1 - k
        down = down - lax.div(chip - down + half, half)
        up = k + lax.div(k - chip + half, half)
        return down + side * (up - down)

    def near_first(k):
        return far_first(half - 2 - k)

    def direct(source, target):
        return (
            ((target > 0) & (target < half - 1))
            | (abs(target - source) <= 1)
            | ((target == 0) & (source == 2))
        )

    def turn(target):
        last = ((chip == 2) & (target == 1)) | (
            (chip == half - 1) & (target == half - 2)
        )
        soon = (core == 1) & ((chip == 0) | ((chip == 2) & (target == 1)))
        return jnp.where(soon, 1, jnp.where(last, 2, 0))

    def direct_count(c):
        return sum(bool(direct(c, t)) for t in range(half) if t != c)

    def relay_count(c):
        return sum(
            2 * (not direct(t, end))
            for end, near in ((0, 1), (half - 1, half - 2))
            for t in range(half)
            if c == near
        )

    def slot(source, target):
        return lax.rem(source - target + half, half) - 1

    piece_at, weight_at = recv_sem.at[0], recv_sem.at[1]

    def join_at(i):
        return recv_sem.at[2 + i]

    def summed_at(owner, target):
        return recv_sem.at[4 + slot(owner, target)]

    partner_at = recv_sem.at[0]

    def total_at(owner):
        return recv_sem.at[1 + owner]

    def shard_at(source, target, i):
        return recv_sem.at[1 + half + 2 * slot(source, target) + i]

    def spread(now):
        for i in range(2):
            for k in range(half - 1):
                target = far_first(k)

                @pl.when(direct(chip, target) & (turn(target) == now))
                def _():
                    send(
                        weights.at[me, i],
                        weights.at[me, i],
                        shard_at(chip, target, i),
                        {"fs": 2 * target},
                    )

    def enter():
        with jax.named_scope("bar"):
            pl.semaphore_wait(barrier, n - 1 + jnp.where(hub, m - 1, 0))

        @pl.when(~hub)
        def _():
            remote(
                own_squares,
                hub_squares.at[me],
                square_sem.at[0],
                square_sem.at[1],
                {"fs": 0},
            ).start()

        spread(0)

        @pl.when(core == 0)
        def _():
            send(weights.at[me], weights.at[me], weight_at, {"fs": partner})

        @pl.when(core == 1)
        def _():
            send(weights.at[me], weights.at[me], partner_at, {"fs": partner})

    with jax.named_scope("cot"):
        landed(cot_v, load_sem.at[0])
    for i in range(2):
        cot_t[pl.ds(i * cols, cols), :] = cot_v[i].T

    for c, (start, size) in enumerate(chunks):
        if c == BARRIER_CHUNK:
            with jax.named_scope("wt"):
                landed(weight_v, load_sem.at[1])
            for i in range(2):
                w = weight_v[i]
                weights[me, i] = w.astype(bf16)
                own_squares[pl.ds(i, 1), :] = jnp.sum(w * w, axis=0, keepdims=True)
            pl.when(chip > 1)(enter)
        if c == BARRIER_CHUNK + 1:
            pl.when(chip == 1)(enter)

        part = pl.ds(start, size)
        with jax.named_scope(f"lat{c}"):
            landed(latent_v.at[:, part], latent_sem.at[c])
        if c == 0:
            load(key_proj, proj_v.at[0], load_sem.at[0])
            load(value_proj, proj_v.at[1], load_sem.at[0])
        if c == BARRIER_CHUNK:
            load(key_first, moment_v.at[0], load_sem.at[1])
            load(key_second, moment_v.at[1], load_sem.at[1])
            load(value_first, moment_v.at[2], load_sem.at[1])
            load(value_second, moment_v.at[3], load_sem.at[1])
        for at in range(start, start + size, DOT_COLS):
            for i in range(2):
                head = pl.ds(i * cols, cols)
                reduced[head, pl.ds(at, DOT_COLS)] = jnp.dot(
                    cot_t[head, :],
                    latent_v[:, pl.ds(at, DOT_COLS)],
                    preferred_element_type=f32,
                ).astype(bf16)
    landed(proj_v, load_sem.at[0])
    totals = [
        jnp.dot(
            reduced[pl.ds(i * cols, cols), :], proj_v[i], preferred_element_type=f32
        )
        for i in range(2)
    ]
    pl.when(chip == 0)(enter)

    def set_scales():
        total = jnp.sum(squares[...], axis=1, keepdims=True)
        scales[...] = jnp.broadcast_to(
            LEARN_RATE * jnp.sqrt(total / entries), scales.shape
        )

    def squares_in():
        with jax.named_scope("sq"):
            arrived(squares, square_sem.at[1])
        set_scales()

    tail = jnp.where(chip == 0, half // 2, 0)

    @pl.when(core == 0)
    def _():
        for i in range(2):
            part = pl.ds(i * rank, rank)
            partial[part, :] = totals[i].astype(bf16).T
            send(partial.at[part], joined.at[part], join_at(i), {"fs": partner})
        shift = jnp.where(chip == 1, 2, jnp.where(chip == half - 2, 1, 0))
        for k in range(half - 1):
            if k == 0:

                @pl.when(hub)
                def _():
                    with jax.named_scope("hub"):
                        arrived(hub_squares.at[pl.ds(1, n - 1)], square_sem.at[1])
                    hub_squares[0] = own_squares[...]
                    tp_squares[mine] = jnp.sum(hub_squares[...], axis=0)
                    for d in range(1, m):
                        remote(
                            tp_squares.at[mine],
                            tp_squares.at[mine],
                            square_sem.at[2],
                            square_sem.at[3],
                            {"tp": lax.rem(mine + d, m)},
                        ).start()

            if k == min(1, half - 2):
                spread(2)

            if k == half - 2:

                @pl.when(hub)
                def _():
                    with jax.named_scope("hubtp"):
                        arrived(tp_squares.at[pl.ds(0, m - 1)], square_sem.at[3])
                    squares[...] = jnp.sum(tp_squares[...], axis=0)
                    for d in range(1, n):
                        remote(
                            squares,
                            squares,
                            square_sem.at[0],
                            square_sem.at[1],
                            {"fs": d},
                        ).start()
                    set_scales()

            origin = near_first(lax.rem(k + shift, half - 1))
            for i in range(2):
                shards = weights.at[pl.ds(2 * origin, 2), i]
                with jax.named_scope(f"w{k}{i}"):
                    arrived(shards, shard_at(origin, chip, i))
                for end, near in ((0, 1), (half - 1, half - 2)):

                    @pl.when((chip == near) & ~direct(origin, end))
                    def _():
                        send(
                            shards, shards, shard_at(origin, end, i), {"fs": 2 * end}
                        )

                send(shards, shards, weight_at, {"fs": partner})
        with jax.named_scope("xw"):
            arrived(weights.at[partner], partner_at)

    @pl.when(core == 1)
    def _():
        for i in range(2):
            turned[i] = totals[i].T
        for i in range(2):
            part = pl.ds(i * rank, rank)
            with jax.named_scope(f"join{i}"):
                arrived(joined.at[part], join_at(i))
            partial[part, :] = (turned[i] + joined[part, :].astype(f32)).astype(bf16)
            for k in range(half - 1):
                target = far_first(lax.rem(k + side, half - 1))
                held_by = jnp.where(target == 0, 1, lax.div(target * piece, rank))

                @pl.when(held_by == i)
                def _():
                    send(
                        partial.at[pl.ds(target * piece, piece)],
                        received.at[slot(chip, target)],
                        piece_at,
                        {"fs": 2 * target + 1},
                    )

        spread(1)
        with jax.named_scope("rs"):
            arrived(received, piece_at)
        own = partial[pl.ds(pl.multiple_of(chip * piece, piece), piece), :]
        gathered[chip] = (
            own.astype(f32) + jnp.sum(received[...].astype(f32), axis=0)
        ).astype(bf16)
        @pl.when(chip == half // 2)
        def _():
            send(gathered.at[chip], gathered.at[chip], total_at(chip), {"fs": 0})

        for k in range(half - 1):
            target = far_first(jnp.where(chip == 0, half - 2 - k, k))
            send(
                gathered.at[chip],
                gathered.at[chip],
                summed_at(chip, target),
                {"fs": 2 * target + 1},
            )
        send(gathered.at[chip], gathered.at[chip], total_at(chip), {"fs": partner})
        spread(2)
        for k in range(half - 1):
            owner = near_first(jnp.where(chip == 1, (k + 1) % (half - 1), k))

            @pl.when(owner != tail)
            def _():
                with jax.named_scope(f"ag{k}"):
                    arrived(gathered.at[owner], summed_at(owner, chip))
                send(
                    gathered.at[owner],
                    gathered.at[owner],
                    total_at(owner),
                    {"fs": partner},
                )

    landed(moment_v, load_sem.at[1])

    def finish(i):
        scale = scales[pl.ds(i, 1), :]
        own_rows = pl.ds(pl.multiple_of(me * rows, rows), rows)
        own_step = scale * steps[i, own_rows, :]
        small[2 + i] = own_step
        small[i] = weight_v[i] - own_step
        held = weights[:, i].astype(f32).reshape(n * rows, cols)
        copied[i] = (held - scale * steps[i]).astype(bf16)

    second = jnp.where(chip == 0, 1, 0)
    here = half // 2
    for turn_of in range(2):
        i = second if turn_of == 1 else 1 - second
        for o in range(here) if turn_of == 0 else reversed(range(here)):
            owner = i * here + o

            @pl.when(core == 0)
            def _():
                with jax.named_scope(f"final{turn_of}{o}"):
                    arrived(gathered.at[owner], total_at(owner))

            if turn_of == 1 and o == 0:

                @pl.when(core == 1)
                def _():
                    with jax.named_scope("aglast"):
                        arrived(gathered.at[tail], summed_at(tail, chip))

                    @pl.when(chip > 0)
                    def _():
                        send(
                            gathered.at[tail],
                            gathered.at[tail],
                            total_at(tail),
                            {"fs": partner},
                        )

            part = pl.ds(o * piece, piece)
            projected = gathered[owner].astype(f32)
            first_new = (
                FIRST_DECAY * moment_v[2 * i, part, :] + (1.0 - FIRST_DECAY) * projected
            )
            second_new = (
                SECOND_DECAY * moment_v[2 * i + 1, part, :]
                + (1.0 - SECOND_DECAY) * projected * projected
            )
            moment[2 * i, part, :] = first_new
            moment[2 * i + 1, part, :] = second_new
            normalized[i, part, :] = (
                first_new / (jnp.sqrt(second_new) + EPSILON)
            ).astype(bf16)

        for at in range(0, width, width // 2):
            some = pl.ds(at, width // 2)
            steps[i, some, :] = jnp.dot(
                proj_v[i, some, :], normalized[i], preferred_element_type=f32
            )

        @pl.when(core == 0)
        def _():
            if turn_of == 0:
                pl.when(~hub)(squares_in)
            finish(i)

        if turn_of == 0:
            pl.when(me == 1)(squares_in)

    @pl.when(core == 1)
    def _():
        with jax.named_scope("fw"):
            arrived(weights.at[pl.ds(0, n - 1)], weight_at)
        pl.when(me > 1)(squares_in)
        for i in range(2):
            finish(i)

    shard_size = 2 * rows * cols
    for c in range(half):
        sent_pieces = 3 * half - 2 + (c == half // 2) - (c == 0)
        shards = [1 + direct_count(c)] * 2
        shards[0] += n - 2 + relay_count(c)

        @pl.when((chip == c) & (core == 0))
        def _():
            all_left(2 * rank * cols + shards[0] * shard_size)

        @pl.when((chip == c) & (core == 1))
        def _():
            all_left(sent_pieces * piece * cols + shards[1] * shard_size)

    @pl.when(hub)
    def _():
        left(tp_squares.at[pl.ds(0, m - 1)], square_sem.at[2])
        left(hub_squares.at[pl.ds(0, n - 1)], square_sem.at[0])

    @pl.when(~hub)
    def _():
        left(own_squares, square_sem.at[0])


def store_kernel(small, moment, copied, *refs):
    outs, sems = refs[:10], refs[10]
    pairs = [(moment.at[i], outs[4 + i], 0) for i in range(4)]
    pairs += [(copied.at[i], outs[8 + i], 1) for i in range(2)]
    pairs += [(small.at[i], outs[i], 2) for i in range(4)]
    for src, out, sem in pairs:
        pltpu.make_async_copy(src, out, sems.at[sem]).start()
    for sem, ref in enumerate((moment, copied, small)):
        pltpu.make_async_copy(ref, ref, sems.at[sem]).wait()


def solution(mesh):
    n, m = mesh.shape["fs"], mesh.shape["tp"]
    half = n // 2

    def body(latent, key_cot, value_cot, key_weight, value_weight, key_proj, *rest):
        f32, bf16 = jnp.float32, jnp.bfloat16
        sds = jax.ShapeDtypeStruct
        tokens, width = latent.shape
        rows, cols = key_weight.shape
        rank = key_proj.shape[1]
        piece = 2 * rank // half
        dma = pltpu.SemaphoreType.DMA
        operands = latent, key_cot, value_cot, key_weight, value_weight, key_proj, *rest
        held = pl.pallas_call(
            functools.partial(exchange_kernel, n, m, float(rows * cols * n * m)),
            out_shape=(
                sds((4, rows, cols), f32),
                sds((4, rank, cols), f32),
                sds((2, n * rows, cols), bf16),
            ),
            in_specs=[HBM] * 11,
            out_specs=(VMEM,) * 3,
            scratch_shapes=[
                pltpu.VMEM((half, piece, cols), bf16),
                pltpu.VMEM((n, 2, rows, cols), bf16),
                pltpu.VMEM((2, rows, cols), f32),
                pltpu.VMEM((2, width, rank), bf16),
                pltpu.VMEM((4, rank, cols), f32),
                pltpu.VMEM((tokens, width), bf16),
                pltpu.VMEM((2, tokens, cols), bf16),
                pltpu.VMEM((2 * cols, tokens), bf16),
                pltpu.VMEM((2 * cols, width), bf16),
                pltpu.VMEM((2 * rank, cols), bf16),
                pltpu.VMEM((2 * rank, cols), bf16),
                pltpu.VMEM((2, rank, cols), f32),
                pltpu.VMEM((2, n * rows, cols), f32),
                pltpu.VMEM((2, rank, cols), bf16),
                pltpu.VMEM((half - 1, piece, cols), bf16),
                pltpu.VMEM((2, cols), f32),
                pltpu.VMEM((n, 2, cols), f32),
                pltpu.VMEM((m, 2, cols), f32),
                pltpu.VMEM((2, cols), f32),
                pltpu.VMEM((2, cols), f32),
                dma((2,)),
                dma((len(CUTS) - 1,)),
                dma,
                dma((3 * half - 1,)),
                dma((4,)),
            ],
            compiler_params=pltpu.CompilerParams(
                collective_id=0, has_side_effects=True, vmem_limit_bytes=24 << 20
            ),
        )(
            *(
                pltpu.with_memory_space_constraint(x, pltpu.MemorySpace.HBM)
                for x in operands
            )
        )
        return pl.pallas_call(
            store_kernel,
            out_shape=(sds((rows, cols), f32),) * 4
            + (sds((rank, cols), f32),) * 4
            + (sds((n * rows, cols), bf16),) * 2,
            in_specs=[VMEM] * 3,
            out_specs=(HBM,) * 10,
            scratch_shapes=[dma((3,))],
            compiler_params=pltpu.CompilerParams(vmem_limit_bytes=24 << 20),
        )(*held)

    split, column = P("fs", "tp"), P(None, "tp")
    return jax.shard_map(
        body,
        mesh=mesh,
        in_specs=(P("fs", None),) + (split,) * 4 + (P(),) * 2 + (column,) * 4,
        out_specs=(split,) * 4 + (column,) * 6,
        check_vma=False,
    )
```

```python
import functools

import jax
import jax.numpy as jnp
from jax import lax
from jax.experimental import pallas as pl
from jax.experimental.pallas import tpu as pltpu
from jax.sharding import PartitionSpec as P

EPSILON = 1e-08
FIRST_DECAY = 0.7
SECOND_DECAY = 0.8
LEARN_RATE = 0.2
CUTS = (0, 1, 2, 4)
BARRIER_CHUNK = 1
DOT_COLS = 256
MESH = pl.DeviceIdType.MESH
HBM = pl.BlockSpec(memory_space=pltpu.MemorySpace.HBM)
VMEM = pl.BlockSpec(memory_space=pltpu.MemorySpace.VMEM)


def exchange_kernel(
    n,
    m,
    entries,
    latent,
    key_cot,
    value_cot,
    key_weight,
    value_weight,
    key_proj,
    value_proj,
    key_first,
    key_second,
    value_first,
    value_second,
    small,
    moment,
    copied,
    gathered,
    weights,
    weight_v,
    proj_v,
    moment_v,
    latent_v,
    cot_v,
    cot_t,
    reduced,
    partial,
    joined,
    turned,
    steps,
    normalized,
    received,
    own_squares,
    hub_squares,
    tp_squares,
    squares,
    scales,
    load_sem,
    latent_sem,
    send_sem,
    recv_sem,
    square_sem,
):
    me = lax.axis_index("fs")
    mine = lax.axis_index("tp")
    core = lax.rem(me, 2)
    chip = lax.div(me, 2)
    partner = me + 1 - 2 * core
    half = n // 2
    width = latent.shape[1]
    rank = key_proj.shape[1]
    rows, cols = key_weight.shape
    piece = gathered.shape[1]
    f32, bf16 = jnp.float32, jnp.bfloat16
    chunks = [
        (a * width // CUTS[-1], (b - a) * width // CUTS[-1])
        for a, b in zip(CUTS, CUTS[1:])
    ]

    def load(src, dst, sem):
        pltpu.make_async_copy(src, dst, sem).start()

    def landed(ref, sem):
        pltpu.make_async_copy(ref, ref, sem).wait()

    load(key_cot, cot_v.at[0], load_sem.at[0])
    load(value_cot, cot_v.at[1], load_sem.at[0])
    for c, (start, size) in enumerate(chunks):
        part = (slice(None), pl.ds(start, size))
        load(latent.at[part], latent_v.at[part], latent_sem.at[c])
        if c == 0:
            load(key_weight, weight_v.at[0], load_sem.at[1])
            load(value_weight, weight_v.at[1], load_sem.at[1])

    barrier = pltpu.get_barrier_semaphore()
    for d in range(1, n):
        pl.semaphore_signal(
            barrier, inc=1, device_id={"fs": lax.rem(me + d, n)}, device_id_type=MESH
        )

    hub = me == 0

    @pl.when(hub)
    def _():
        for d in range(1, m):
            pl.semaphore_signal(
                barrier,
                inc=1,
                device_id={"tp": lax.rem(mine + d, m)},
                device_id_type=MESH,
            )

    def remote(src, dst, sem, arrival, where):
        return pltpu.make_async_remote_copy(
            src_ref=src,
            dst_ref=dst,
            send_sem=sem,
            recv_sem=arrival,
            device_id=where,
            device_id_type=MESH,
        )

    def send(src, dst, arrival, where):
        remote(src, dst, send_sem, arrival, where).start()

    def arrived(ref, sem):
        remote(ref, ref, sem, sem, {"fs": partner}).wait_recv()

    def left(ref, sem):
        remote(ref, ref, sem, sem, {"fs": partner}).wait_send()

    def all_left(elements):
        across = next(
            w
            for w in (width, width // 2, width // 4, width // 8)
            if elements % (16 * w) == 0 and elements <= w * latent_v.shape[0]
        )
        left(latent_v.at[pl.ds(0, elements // across), pl.ds(0, across)], send_sem)

    side = lax.div(chip, (half + 1) // 2)

    def far_first(k):
        down = half - 1 - k
        down = down - lax.div(chip - down + half, half)
        up = k + lax.div(k - chip + half, half)
        return down + side * (up - down)

    def near_first(k):
        return far_first(half - 2 - k)

    def direct(source, target):
        return (
            ((target > 0) & (target < half - 1))
            | (abs(target - source) <= 1)
            | ((target == 0) & (source == 2))
        )

    def turn(target):
        last = ((chip == 2) & (target == 1)) | (
            (chip == half - 1) & (target == half - 2)
        )
        soon = (core == 1) & ((chip == 0) | ((chip == 2) & (target == 1)))
        return jnp.where(soon, 1, jnp.where(last, 2, 0))

    def direct_count(c):
        return sum(bool(direct(c, t)) for t in range(half) if t != c)

    def relay_count(c):
        return sum(
            2 * (not direct(t, end))
            for end, near in ((0, 1), (half - 1, half - 2))
            for t in range(half)
            if c == near
        )

    def slot(source, target):
        return lax.rem(source - target + half, half) - 1

    piece_at, weight_at = recv_sem.at[0], recv_sem.at[1]

    def join_at(t):
        return recv_sem.at[2 + t]

    def summed_at(owner, target):
        return recv_sem.at[2 + half + slot(owner, target)]

    partner_at = recv_sem.at[0]

    def total_at(owner):
        return recv_sem.at[1 + owner]

    def shard_at(source, target, i):
        return recv_sem.at[1 + half + 2 * slot(source, target) + i]

    def spread(now):
        for i in range(2):
            for k in range(half - 1):
                target = far_first(k)

                @pl.when(direct(chip, target) & (turn(target) == now))
                def _():
                    send(
                        weights.at[me, i],
                        weights.at[me, i],
                        shard_at(chip, target, i),
                        {"fs": 2 * target},
                    )

    def enter():
        with jax.named_scope("bar"):
            pl.semaphore_wait(barrier, n - 1 + jnp.where(hub, m - 1, 0))

        @pl.when(~hub)
        def _():
            remote(
                own_squares,
                hub_squares.at[me],
                square_sem.at[0],
                square_sem.at[1],
                {"fs": 0},
            ).start()

        spread(0)

        @pl.when(core == 0)
        def _():
            send(weights.at[me], weights.at[me], weight_at, {"fs": partner})

        @pl.when(core == 1)
        def _():
            send(weights.at[me], weights.at[me], partner_at, {"fs": partner})

    with jax.named_scope("cot"):
        landed(cot_v, load_sem.at[0])
    for i in range(2):
        cot_t[pl.ds(i * cols, cols), :] = cot_v[i].T

    for c, (start, size) in enumerate(chunks):
        if c == BARRIER_CHUNK:
            with jax.named_scope("wt"):
                landed(weight_v, load_sem.at[1])
            for i in range(2):
                w = weight_v[i]
                weights[me, i] = w.astype(bf16)
                own_squares[pl.ds(i, 1), :] = jnp.sum(w * w, axis=0, keepdims=True)
            pl.when(chip > 1)(enter)
        if c == BARRIER_CHUNK + 1:
            pl.when(chip == 1)(enter)

        part = pl.ds(start, size)
        with jax.named_scope(f"lat{c}"):
            landed(latent_v.at[:, part], latent_sem.at[c])
        if c == 0:
            load(key_proj, proj_v.at[0], load_sem.at[0])
            load(value_proj, proj_v.at[1], load_sem.at[0])
        if c == BARRIER_CHUNK:
            load(key_first, moment_v.at[0], load_sem.at[1])
            load(key_second, moment_v.at[1], load_sem.at[1])
            load(value_first, moment_v.at[2], load_sem.at[1])
            load(value_second, moment_v.at[3], load_sem.at[1])
        for at in range(start, start + size, DOT_COLS):
            for i in range(2):
                head = pl.ds(i * cols, cols)
                reduced[head, pl.ds(at, DOT_COLS)] = jnp.dot(
                    cot_t[head, :],
                    latent_v[:, pl.ds(at, DOT_COLS)],
                    preferred_element_type=f32,
                ).astype(bf16)
    landed(proj_v, load_sem.at[0])
    totals = [
        jnp.dot(
            reduced[pl.ds(i * cols, cols), :], proj_v[i], preferred_element_type=f32
        )
        for i in range(2)
    ]
    pl.when(chip == 0)(enter)

    def set_scales():
        total = jnp.sum(squares[...], axis=1, keepdims=True)
        scales[...] = jnp.broadcast_to(
            LEARN_RATE * jnp.sqrt(total / entries), scales.shape
        )

    def squares_in():
        with jax.named_scope("sq"):
            arrived(squares, square_sem.at[1])
        set_scales()

    urgent = (*range(1, half), 0)
    tail = jnp.where(chip == 0, half // 2, 0)

    @pl.when(core == 0)
    def _():
        for i in range(2):
            partial[pl.ds(i * rank, rank), :] = totals[i].astype(bf16).T
            for t in urgent:
                if (1 if t == 0 else t * piece // rank) == i:
                    part = pl.ds(t * piece, piece)
                    send(
                        partial.at[part], joined.at[part], join_at(t), {"fs": partner}
                    )

        shift = jnp.where(chip == 1, 2, jnp.where(chip == half - 2, 1, 0))
        for k in range(half - 1):
            if k == 0:

                @pl.when(hub)
                def _():
                    with jax.named_scope("hub"):
                        arrived(hub_squares.at[pl.ds(1, n - 1)], square_sem.at[1])
                    hub_squares[0] = own_squares[...]
                    tp_squares[mine] = jnp.sum(hub_squares[...], axis=0)
                    for d in range(1, m):
                        remote(
                            tp_squares.at[mine],
                            tp_squares.at[mine],
                            square_sem.at[2],
                            square_sem.at[3],
                            {"tp": lax.rem(mine + d, m)},
                        ).start()

            if k == min(1, half - 2):
                spread(2)

            if k == half - 2:

                @pl.when(hub)
                def _():
                    with jax.named_scope("hubtp"):
                        arrived(tp_squares.at[pl.ds(0, m - 1)], square_sem.at[3])
                    squares[...] = jnp.sum(tp_squares[...], axis=0)
                    for d in range(1, n):
                        remote(
                            squares,
                            squares,
                            square_sem.at[0],
                            square_sem.at[1],
                            {"fs": d},
                        ).start()
                    set_scales()

            origin = near_first(lax.rem(k + shift, half - 1))
            for i in range(2):
                shards = weights.at[pl.ds(2 * origin, 2), i]
                with jax.named_scope(f"w{k}{i}"):
                    arrived(shards, shard_at(origin, chip, i))
                for end, near in ((0, 1), (half - 1, half - 2)):

                    @pl.when((chip == near) & ~direct(origin, end))
                    def _():
                        send(
                            shards, shards, shard_at(origin, end, i), {"fs": 2 * end}
                        )

                send(shards, shards, weight_at, {"fs": partner})
        with jax.named_scope("xw"):
            arrived(weights.at[partner], partner_at)

    @pl.when(core == 1)
    def _():
        for i in range(2):
            turned[pl.ds(i * rank, rank), :] = totals[i].T
        for k, late in enumerate(urgent):
            t = jnp.where((side == 0) & (late > 0), half - 1 - k, late)
            part = pl.ds(pl.multiple_of(t * piece, piece), piece)
            with jax.named_scope(f"join{k}"):
                arrived(joined.at[part], join_at(t))
            partial[part, :] = (turned[part, :] + joined[part, :].astype(f32)).astype(
                bf16
            )

            @pl.when(chip != t)
            def _():
                send(
                    partial.at[part],
                    received.at[slot(chip, t)],
                    piece_at,
                    {"fs": 2 * t + 1},
                )

        spread(1)
        with jax.named_scope("rs"):
            arrived(received, piece_at)
        own = partial[pl.ds(pl.multiple_of(chip * piece, piece), piece), :]
        gathered[chip] = (
            own.astype(f32) + jnp.sum(received[...].astype(f32), axis=0)
        ).astype(bf16)
        @pl.when((chip == 1) | (chip == half // 2))
        def _():
            send(gathered.at[chip], gathered.at[chip], total_at(chip), {"fs": 0})

        for k in range(half - 1):
            target = far_first(jnp.where(chip == 0, half - 2 - k, k))
            send(
                gathered.at[chip],
                gathered.at[chip],
                summed_at(chip, target),
                {"fs": 2 * target + 1},
            )
        send(gathered.at[chip], gathered.at[chip], total_at(chip), {"fs": partner})
        spread(2)
        for k in range(half - 1):
            place = jnp.where(chip == 0, half - 2 - k, k)
            owner = near_first(jnp.where(chip == 1, (k + 1) % (half - 1), place))

            @pl.when(owner != tail)
            def _():
                with jax.named_scope(f"ag{k}"):
                    arrived(gathered.at[owner], summed_at(owner, chip))

                @pl.when((chip > 0) | (owner != 1))
                def _():
                    send(
                        gathered.at[owner],
                        gathered.at[owner],
                        total_at(owner),
                        {"fs": partner},
                    )

    landed(moment_v, load_sem.at[1])

    def finish(i):
        scale = scales[pl.ds(i, 1), :]
        own_rows = pl.ds(pl.multiple_of(me * rows, rows), rows)
        own_step = scale * steps[i, own_rows, :]
        small[2 + i] = own_step
        small[i] = weight_v[i] - own_step
        held = weights[:, i].astype(f32).reshape(n * rows, cols)
        copied[i] = (held - scale * steps[i]).astype(bf16)

    second = jnp.where(chip == 0, 1, 0)
    here = half // 2
    for turn_of in range(2):
        i = second if turn_of == 1 else 1 - second
        for o in range(here) if turn_of == 0 else reversed(range(here)):
            owner = i * here + o

            @pl.when(core == 0)
            def _():
                with jax.named_scope(f"final{turn_of}{o}"):
                    arrived(gathered.at[owner], total_at(owner))

            if turn_of == 1 and o == 0:

                @pl.when(core == 1)
                def _():
                    with jax.named_scope("aglast"):
                        arrived(gathered.at[tail], summed_at(tail, chip))

                    @pl.when(chip > 0)
                    def _():
                        send(
                            gathered.at[tail],
                            gathered.at[tail],
                            total_at(tail),
                            {"fs": partner},
                        )

            part = pl.ds(o * piece, piece)
            projected = gathered[owner].astype(f32)
            first_new = (
                FIRST_DECAY * moment_v[2 * i, part, :] + (1.0 - FIRST_DECAY) * projected
            )
            second_new = (
                SECOND_DECAY * moment_v[2 * i + 1, part, :]
                + (1.0 - SECOND_DECAY) * projected * projected
            )
            moment[2 * i, part, :] = first_new
            moment[2 * i + 1, part, :] = second_new
            normalized[i, part, :] = (
                first_new / (jnp.sqrt(second_new) + EPSILON)
            ).astype(bf16)

        for at in range(0, width, width // 2):
            some = pl.ds(at, width // 2)
            steps[i, some, :] = jnp.dot(
                proj_v[i, some, :], normalized[i], preferred_element_type=f32
            )

        @pl.when(core == 0)
        def _():
            if turn_of == 0:
                pl.when(~hub)(squares_in)
            finish(i)

        if turn_of == 0:
            pl.when(me == 1)(squares_in)

    @pl.when(core == 1)
    def _():
        with jax.named_scope("fw"):
            arrived(weights.at[pl.ds(0, n - 1)], weight_at)
        pl.when(me > 1)(squares_in)
        for i in range(2):
            finish(i)

    shard_size = 2 * rows * cols
    for c in range(half):
        to_both = {1, half // 2}
        sent_pieces = 3 * half - 2 + (c in to_both) - (c == 0) * len(to_both)
        shards = [1 + direct_count(c)] * 2
        shards[0] += n - 2 + relay_count(c)

        @pl.when((chip == c) & (core == 0))
        def _():
            all_left(2 * rank * cols + shards[0] * shard_size)

        @pl.when((chip == c) & (core == 1))
        def _():
            all_left(sent_pieces * piece * cols + shards[1] * shard_size)

    @pl.when(hub)
    def _():
        left(tp_squares.at[pl.ds(0, m - 1)], square_sem.at[2])
        left(hub_squares.at[pl.ds(0, n - 1)], square_sem.at[0])

    @pl.when(~hub)
    def _():
        left(own_squares, square_sem.at[0])


def store_kernel(small, moment, copied, *refs):
    outs, sems = refs[:10], refs[10]
    pairs = [(moment.at[i], outs[4 + i], 0) for i in range(4)]
    pairs += [(copied.at[i], outs[8 + i], 1) for i in range(2)]
    pairs += [(small.at[i], outs[i], 2) for i in range(4)]
    for src, out, sem in pairs:
        pltpu.make_async_copy(src, out, sems.at[sem]).start()
    for sem, ref in enumerate((moment, copied, small)):
        pltpu.make_async_copy(ref, ref, sems.at[sem]).wait()


def solution(mesh):
    n, m = mesh.shape["fs"], mesh.shape["tp"]
    half = n // 2

    def body(latent, key_cot, value_cot, key_weight, value_weight, key_proj, *rest):
        f32, bf16 = jnp.float32, jnp.bfloat16
        sds = jax.ShapeDtypeStruct
        tokens, width = latent.shape
        rows, cols = key_weight.shape
        rank = key_proj.shape[1]
        piece = 2 * rank // half
        dma = pltpu.SemaphoreType.DMA
        operands = latent, key_cot, value_cot, key_weight, value_weight, key_proj, *rest
        held = pl.pallas_call(
            functools.partial(exchange_kernel, n, m, float(rows * cols * n * m)),
            out_shape=(
                sds((4, rows, cols), f32),
                sds((4, rank, cols), f32),
                sds((2, n * rows, cols), bf16),
            ),
            in_specs=[HBM] * 11,
            out_specs=(VMEM,) * 3,
            scratch_shapes=[
                pltpu.VMEM((half, piece, cols), bf16),
                pltpu.VMEM((n, 2, rows, cols), bf16),
                pltpu.VMEM((2, rows, cols), f32),
                pltpu.VMEM((2, width, rank), bf16),
                pltpu.VMEM((4, rank, cols), f32),
                pltpu.VMEM((tokens, width), bf16),
                pltpu.VMEM((2, tokens, cols), bf16),
                pltpu.VMEM((2 * cols, tokens), bf16),
                pltpu.VMEM((2 * cols, width), bf16),
                pltpu.VMEM((2 * rank, cols), bf16),
                pltpu.VMEM((2 * rank, cols), bf16),
                pltpu.VMEM((2 * rank, cols), f32),
                pltpu.VMEM((2, n * rows, cols), f32),
                pltpu.VMEM((2, rank, cols), bf16),
                pltpu.VMEM((half - 1, piece, cols), bf16),
                pltpu.VMEM((2, cols), f32),
                pltpu.VMEM((n, 2, cols), f32),
                pltpu.VMEM((m, 2, cols), f32),
                pltpu.VMEM((2, cols), f32),
                pltpu.VMEM((2, cols), f32),
                dma((2,)),
                dma((len(CUTS) - 1,)),
                dma,
                dma((3 * half - 1,)),
                dma((4,)),
            ],
            compiler_params=pltpu.CompilerParams(
                collective_id=0, has_side_effects=True, vmem_limit_bytes=24 << 20
            ),
        )(
            *(
                pltpu.with_memory_space_constraint(x, pltpu.MemorySpace.HBM)
                for x in operands
            )
        )
        return pl.pallas_call(
            store_kernel,
            out_shape=(sds((rows, cols), f32),) * 4
            + (sds((rank, cols), f32),) * 4
            + (sds((n * rows, cols), bf16),) * 2,
            in_specs=[VMEM] * 3,
            out_specs=(HBM,) * 10,
            scratch_shapes=[dma((3,))],
            compiler_params=pltpu.CompilerParams(vmem_limit_bytes=24 << 20),
        )(*held)

    split, column = P("fs", "tp"), P(None, "tp")
    return jax.shard_map(
        body,
        mesh=mesh,
        in_specs=(P("fs", None),) + (split,) * 4 + (P(),) * 2 + (column,) * 4,
        out_specs=(split,) * 4 + (column,) * 6,
        check_vma=False,
    )
```

```python
import functools

import jax
import jax.numpy as jnp
from jax import lax
from jax.experimental import pallas as pl
from jax.experimental.pallas import tpu as pltpu
from jax.sharding import PartitionSpec as P

EPSILON = 1e-08
FIRST_DECAY = 0.7
SECOND_DECAY = 0.8
LEARN_RATE = 0.2
CUTS = (0, 1, 2, 4)
BARRIER_CHUNK = 1
DOT_COLS = 256
MESH = pl.DeviceIdType.MESH
HBM = pl.BlockSpec(memory_space=pltpu.MemorySpace.HBM)
VMEM = pl.BlockSpec(memory_space=pltpu.MemorySpace.VMEM)


def exchange_kernel(
    n,
    m,
    entries,
    latent,
    key_cot,
    value_cot,
    key_weight,
    value_weight,
    key_proj,
    value_proj,
    key_first,
    key_second,
    value_first,
    value_second,
    small,
    moment,
    copied,
    gathered,
    weights,
    weight_v,
    proj_v,
    moment_v,
    latent_v,
    cot_v,
    cot_t,
    reduced,
    partial,
    joined,
    turned,
    steps,
    normalized,
    received,
    own_squares,
    hub_squares,
    tp_squares,
    squares,
    scales,
    load_sem,
    latent_sem,
    send_sem,
    recv_sem,
    square_sem,
):
    me = lax.axis_index("fs")
    mine = lax.axis_index("tp")
    core = lax.rem(me, 2)
    chip = lax.div(me, 2)
    partner = me + 1 - 2 * core
    half = n // 2
    width = latent.shape[1]
    rank = key_proj.shape[1]
    rows, cols = key_weight.shape
    piece = gathered.shape[1]
    f32, bf16 = jnp.float32, jnp.bfloat16
    chunks = [
        (a * width // CUTS[-1], (b - a) * width // CUTS[-1])
        for a, b in zip(CUTS, CUTS[1:])
    ]

    def load(src, dst, sem):
        pltpu.make_async_copy(src, dst, sem).start()

    def landed(ref, sem):
        pltpu.make_async_copy(ref, ref, sem).wait()

    load(key_cot, cot_v.at[0], load_sem.at[0])
    load(value_cot, cot_v.at[1], load_sem.at[0])
    for c, (start, size) in enumerate(chunks):
        part = (slice(None), pl.ds(start, size))
        load(latent.at[part], latent_v.at[part], latent_sem.at[c])
        if c == 0:
            load(key_weight, weight_v.at[0], load_sem.at[1])
            load(value_weight, weight_v.at[1], load_sem.at[1])

    barrier = pltpu.get_barrier_semaphore()
    for d in range(1, n):
        pl.semaphore_signal(
            barrier, inc=1, device_id={"fs": lax.rem(me + d, n)}, device_id_type=MESH
        )

    hub = me == 0

    @pl.when(hub)
    def _():
        for d in range(1, m):
            pl.semaphore_signal(
                barrier,
                inc=1,
                device_id={"tp": lax.rem(mine + d, m)},
                device_id_type=MESH,
            )

    def remote(src, dst, sem, arrival, where):
        return pltpu.make_async_remote_copy(
            src_ref=src,
            dst_ref=dst,
            send_sem=sem,
            recv_sem=arrival,
            device_id=where,
            device_id_type=MESH,
        )

    def send(src, dst, arrival, where):
        remote(src, dst, send_sem, arrival, where).start()

    def arrived(ref, sem):
        remote(ref, ref, sem, sem, {"fs": partner}).wait_recv()

    def left(ref, sem):
        remote(ref, ref, sem, sem, {"fs": partner}).wait_send()

    def all_left(elements):
        across = next(
            w
            for w in (width, width // 2, width // 4, width // 8)
            if elements % (16 * w) == 0 and elements <= w * latent_v.shape[0]
        )
        left(latent_v.at[pl.ds(0, elements // across), pl.ds(0, across)], send_sem)

    side = lax.div(chip, (half + 1) // 2)

    def far_first(k):
        down = half - 1 - k
        down = down - lax.div(chip - down + half, half)
        up = k + lax.div(k - chip + half, half)
        return down + side * (up - down)

    def near_first(k):
        return far_first(half - 2 - k)

    def direct(source, target):
        return (
            ((target > 0) & (target < half - 1))
            | (abs(target - source) <= 1)
            | ((target == 0) & (source == 2))
        )

    def turn(target):
        last = ((chip == 2) & (target == 1)) | (
            (chip == half - 1) & (target == half - 2)
        )
        soon = (core == 1) & ((chip == 0) | ((chip == 2) & (target == 1)))
        return jnp.where(soon, 1, jnp.where(last, 2, 0))

    def direct_count(c):
        return sum(bool(direct(c, t)) for t in range(half) if t != c)

    def relay_count(c):
        return sum(
            2 * (not direct(t, end))
            for end, near in ((0, 1), (half - 1, half - 2))
            for t in range(half)
            if c == near
        )

    def slot(source, target):
        return lax.rem(source - target + half, half) - 1

    piece_at, weight_at = recv_sem.at[0], recv_sem.at[1]

    def join_at(t):
        return recv_sem.at[2 + t]

    def summed_at(owner, target):
        return recv_sem.at[2 + half + slot(owner, target)]

    partner_at = recv_sem.at[0]

    def total_at(owner):
        return recv_sem.at[1 + owner]

    def shard_at(source, target, i):
        return recv_sem.at[1 + half + 2 * slot(source, target) + i]

    def spread(now):
        for i in range(2):
            for k in range(half - 1):
                target = far_first(k)

                @pl.when(direct(chip, target) & (turn(target) == now))
                def _():
                    send(
                        weights.at[me, i],
                        weights.at[me, i],
                        shard_at(chip, target, i),
                        {"fs": 2 * target},
                    )

    def enter():
        with jax.named_scope("bar"):
            pl.semaphore_wait(barrier, n - 1 + jnp.where(hub, m - 1, 0))

        @pl.when(~hub)
        def _():
            remote(
                own_squares,
                hub_squares.at[me],
                square_sem.at[0],
                square_sem.at[1],
                {"fs": 0},
            ).start()

        spread(0)

        @pl.when(core == 0)
        def _():
            send(weights.at[me], weights.at[me], weight_at, {"fs": partner})

        @pl.when(core == 1)
        def _():
            send(weights.at[me], weights.at[me], partner_at, {"fs": partner})

    with jax.named_scope("cot"):
        landed(cot_v, load_sem.at[0])
    for i in range(2):
        cot_t[pl.ds(i * cols, cols), :] = cot_v[i].T

    for c, (start, size) in enumerate(chunks):
        if c == BARRIER_CHUNK:
            with jax.named_scope("wt"):
                landed(weight_v, load_sem.at[1])
            for i in range(2):
                w = weight_v[i]
                weights[me, i] = w.astype(bf16)
                own_squares[pl.ds(i, 1), :] = jnp.sum(w * w, axis=0, keepdims=True)
            pl.when(chip > 1)(enter)
        if c == BARRIER_CHUNK + 1:
            pl.when(chip == 1)(enter)

        part = pl.ds(start, size)
        with jax.named_scope(f"lat{c}"):
            landed(latent_v.at[:, part], latent_sem.at[c])
        if c == 0:
            load(key_proj, proj_v.at[0], load_sem.at[0])
            load(value_proj, proj_v.at[1], load_sem.at[0])
        if c == BARRIER_CHUNK:
            load(key_first, moment_v.at[0], load_sem.at[1])
            load(key_second, moment_v.at[1], load_sem.at[1])
            load(value_first, moment_v.at[2], load_sem.at[1])
            load(value_second, moment_v.at[3], load_sem.at[1])
        for at in range(start, start + size, DOT_COLS):
            for i in range(2):
                head = pl.ds(i * cols, cols)
                reduced[head, pl.ds(at, DOT_COLS)] = jnp.dot(
                    cot_t[head, :],
                    latent_v[:, pl.ds(at, DOT_COLS)],
                    preferred_element_type=f32,
                ).astype(bf16)
    landed(proj_v, load_sem.at[0])
    totals = [
        jnp.dot(
            reduced[pl.ds(i * cols, cols), :], proj_v[i], preferred_element_type=f32
        )
        for i in range(2)
    ]
    pl.when(chip == 0)(enter)

    def set_scales():
        total = jnp.sum(squares[...], axis=1, keepdims=True)
        scales[...] = jnp.broadcast_to(
            LEARN_RATE * jnp.sqrt(total / entries), scales.shape
        )

    def squares_in():
        with jax.named_scope("sq"):
            arrived(squares, square_sem.at[1])
        set_scales()

    urgent = (*range(1, half), 0)
    tail = jnp.where(chip == 0, half // 2, 0)

    @pl.when(core == 0)
    def _():
        for i in range(2):
            partial[pl.ds(i * rank, rank), :] = totals[i].astype(bf16).T
            for t in urgent:
                if (1 if t == 0 else t * piece // rank) == i:
                    part = pl.ds(t * piece, piece)
                    send(
                        partial.at[part], joined.at[part], join_at(t), {"fs": partner}
                    )

        shift = jnp.where(chip == 1, 2, jnp.where(chip == half - 2, 1, 0))
        for k in range(half - 1):
            if k == 0:

                @pl.when(hub)
                def _():
                    with jax.named_scope("hub"):
                        arrived(hub_squares.at[pl.ds(1, n - 1)], square_sem.at[1])
                    hub_squares[0] = own_squares[...]
                    tp_squares[mine] = jnp.sum(hub_squares[...], axis=0)
                    for d in range(1, m):
                        remote(
                            tp_squares.at[mine],
                            tp_squares.at[mine],
                            square_sem.at[2],
                            square_sem.at[3],
                            {"tp": lax.rem(mine + d, m)},
                        ).start()

            if k == min(1, half - 2):
                spread(2)

            if k == half - 2:

                @pl.when(hub)
                def _():
                    with jax.named_scope("hubtp"):
                        arrived(tp_squares.at[pl.ds(0, m - 1)], square_sem.at[3])
                    squares[...] = jnp.sum(tp_squares[...], axis=0)
                    for d in range(1, n):
                        remote(
                            squares,
                            squares,
                            square_sem.at[0],
                            square_sem.at[1],
                            {"fs": d},
                        ).start()
                    set_scales()

            origin = near_first(lax.rem(k + shift, half - 1))
            for i in range(2):
                shards = weights.at[pl.ds(2 * origin, 2), i]
                with jax.named_scope(f"w{k}{i}"):
                    arrived(shards, shard_at(origin, chip, i))
                for end, near in ((0, 1), (half - 1, half - 2)):

                    @pl.when((chip == near) & ~direct(origin, end))
                    def _():
                        send(
                            shards, shards, shard_at(origin, end, i), {"fs": 2 * end}
                        )

                send(shards, shards, weight_at, {"fs": partner})
        with jax.named_scope("xw"):
            arrived(weights.at[partner], partner_at)

    @pl.when(core == 1)
    def _():
        for i in range(2):
            turned[pl.ds(i * rank, rank), :] = totals[i].T
        for k, late in enumerate(urgent):
            t = jnp.where((side == 0) & (late > 0), half - 1 - k, late)
            part = pl.ds(pl.multiple_of(t * piece, piece), piece)
            with jax.named_scope(f"join{k}"):
                arrived(joined.at[part], join_at(t))
            partial[part, :] = (turned[part, :] + joined[part, :].astype(f32)).astype(
                bf16
            )

            @pl.when(chip != t)
            def _():
                send(
                    partial.at[part],
                    received.at[slot(chip, t)],
                    piece_at,
                    {"fs": 2 * t + 1},
                )

        spread(1)
        with jax.named_scope("rs"):
            arrived(received, piece_at)
        own = partial[pl.ds(pl.multiple_of(chip * piece, piece), piece), :]
        gathered[chip] = (
            own.astype(f32) + jnp.sum(received[...].astype(f32), axis=0)
        ).astype(bf16)
        for k in range(half - 1):
            target = far_first(jnp.where(chip == 0, half - 2 - k, k))
            send(
                gathered.at[chip],
                gathered.at[chip],
                summed_at(chip, target),
                {"fs": 2 * target + 1},
            )

            @pl.when((target == 0) & ((chip == 1) | (chip == half // 2)))
            def _():
                send(gathered.at[chip], gathered.at[chip], total_at(chip), {"fs": 0})

        send(gathered.at[chip], gathered.at[chip], total_at(chip), {"fs": partner})
        spread(2)
        for k in range(half - 1):
            place = jnp.where(chip == 0, half - 2 - k, k)
            owner = near_first(jnp.where(chip == 1, (k + 1) % (half - 1), place))

            @pl.when(owner != tail)
            def _():
                with jax.named_scope(f"ag{k}"):
                    arrived(gathered.at[owner], summed_at(owner, chip))

                @pl.when((chip > 0) | (owner != 1))
                def _():
                    send(
                        gathered.at[owner],
                        gathered.at[owner],
                        total_at(owner),
                        {"fs": partner},
                    )

    landed(moment_v, load_sem.at[1])

    def finish(i):
        scale = scales[pl.ds(i, 1), :]
        own_rows = pl.ds(pl.multiple_of(me * rows, rows), rows)
        own_step = scale * steps[i, own_rows, :]
        small[2 + i] = own_step
        small[i] = weight_v[i] - own_step
        held = weights[:, i].astype(f32).reshape(n * rows, cols)
        copied[i] = (held - scale * steps[i]).astype(bf16)

    second = jnp.where(chip == 0, 1, 0)
    here = half // 2
    for turn_of in range(2):
        i = second if turn_of == 1 else 1 - second
        for o in range(here) if turn_of == 0 else reversed(range(here)):
            owner = i * here + o

            @pl.when(core == 0)
            def _():
                with jax.named_scope(f"final{turn_of}{o}"):
                    arrived(gathered.at[owner], total_at(owner))

            if turn_of == 1 and o == 0:

                @pl.when(core == 1)
                def _():
                    with jax.named_scope("aglast"):
                        arrived(gathered.at[tail], summed_at(tail, chip))

                    @pl.when(chip > 0)
                    def _():
                        send(
                            gathered.at[tail],
                            gathered.at[tail],
                            total_at(tail),
                            {"fs": partner},
                        )

            part = pl.ds(o * piece, piece)
            projected = gathered[owner].astype(f32)
            first_new = (
                FIRST_DECAY * moment_v[2 * i, part, :] + (1.0 - FIRST_DECAY) * projected
            )
            second_new = (
                SECOND_DECAY * moment_v[2 * i + 1, part, :]
                + (1.0 - SECOND_DECAY) * projected * projected
            )
            moment[2 * i, part, :] = first_new
            moment[2 * i + 1, part, :] = second_new
            normalized[i, part, :] = (
                first_new / (jnp.sqrt(second_new) + EPSILON)
            ).astype(bf16)

        for at in range(0, width, width // 2):
            some = pl.ds(at, width // 2)
            steps[i, some, :] = jnp.dot(
                proj_v[i, some, :], normalized[i], preferred_element_type=f32
            )

        @pl.when(core == 0)
        def _():
            if turn_of == 0:
                pl.when(~hub)(squares_in)
            finish(i)

        if turn_of == 0:
            pl.when(me == 1)(squares_in)

    @pl.when(core == 1)
    def _():
        with jax.named_scope("fw"):
            arrived(weights.at[pl.ds(0, n - 1)], weight_at)
        pl.when(me > 1)(squares_in)
        for i in range(2):
            finish(i)

    shard_size = 2 * rows * cols
    for c in range(half):
        to_both = {1, half // 2}
        sent_pieces = 3 * half - 2 + (c in to_both) - (c == 0) * len(to_both)
        shards = [1 + direct_count(c)] * 2
        shards[0] += n - 2 + relay_count(c)

        @pl.when((chip == c) & (core == 0))
        def _():
            all_left(2 * rank * cols + shards[0] * shard_size)

        @pl.when((chip == c) & (core == 1))
        def _():
            all_left(sent_pieces * piece * cols + shards[1] * shard_size)

    @pl.when(hub)
    def _():
        left(tp_squares.at[pl.ds(0, m - 1)], square_sem.at[2])
        left(hub_squares.at[pl.ds(0, n - 1)], square_sem.at[0])

    @pl.when(~hub)
    def _():
        left(own_squares, square_sem.at[0])


def store_kernel(small, moment, copied, *refs):
    outs, sems = refs[:10], refs[10]
    pairs = [(moment.at[i], outs[4 + i], 0) for i in range(4)]
    pairs += [(copied.at[i], outs[8 + i], 1) for i in range(2)]
    pairs += [(small.at[i], outs[i], 2) for i in range(4)]
    for src, out, sem in pairs:
        pltpu.make_async_copy(src, out, sems.at[sem]).start()
    for sem, ref in enumerate((moment, copied, small)):
        pltpu.make_async_copy(ref, ref, sems.at[sem]).wait()


def solution(mesh):
    n, m = mesh.shape["fs"], mesh.shape["tp"]
    half = n // 2

    def body(latent, key_cot, value_cot, key_weight, value_weight, key_proj, *rest):
        f32, bf16 = jnp.float32, jnp.bfloat16
        sds = jax.ShapeDtypeStruct
        tokens, width = latent.shape
        rows, cols = key_weight.shape
        rank = key_proj.shape[1]
        piece = 2 * rank // half
        dma = pltpu.SemaphoreType.DMA
        operands = latent, key_cot, value_cot, key_weight, value_weight, key_proj, *rest
        held = pl.pallas_call(
            functools.partial(exchange_kernel, n, m, float(rows * cols * n * m)),
            out_shape=(
                sds((4, rows, cols), f32),
                sds((4, rank, cols), f32),
                sds((2, n * rows, cols), bf16),
            ),
            in_specs=[HBM] * 11,
            out_specs=(VMEM,) * 3,
            scratch_shapes=[
                pltpu.VMEM((half, piece, cols), bf16),
                pltpu.VMEM((n, 2, rows, cols), bf16),
                pltpu.VMEM((2, rows, cols), f32),
                pltpu.VMEM((2, width, rank), bf16),
                pltpu.VMEM((4, rank, cols), f32),
                pltpu.VMEM((tokens, width), bf16),
                pltpu.VMEM((2, tokens, cols), bf16),
                pltpu.VMEM((2 * cols, tokens), bf16),
                pltpu.VMEM((2 * cols, width), bf16),
                pltpu.VMEM((2 * rank, cols), bf16),
                pltpu.VMEM((2 * rank, cols), bf16),
                pltpu.VMEM((2 * rank, cols), f32),
                pltpu.VMEM((2, n * rows, cols), f32),
                pltpu.VMEM((2, rank, cols), bf16),
                pltpu.VMEM((half - 1, piece, cols), bf16),
                pltpu.VMEM((2, cols), f32),
                pltpu.VMEM((n, 2, cols), f32),
                pltpu.VMEM((m, 2, cols), f32),
                pltpu.VMEM((2, cols), f32),
                pltpu.VMEM((2, cols), f32),
                dma((2,)),
                dma((len(CUTS) - 1,)),
                dma,
                dma((3 * half - 1,)),
                dma((4,)),
            ],
            compiler_params=pltpu.CompilerParams(
                collective_id=0, has_side_effects=True, vmem_limit_bytes=24 << 20
            ),
        )(
            *(
                pltpu.with_memory_space_constraint(x, pltpu.MemorySpace.HBM)
                for x in operands
            )
        )
        return pl.pallas_call(
            store_kernel,
            out_shape=(sds((rows, cols), f32),) * 4
            + (sds((rank, cols), f32),) * 4
            + (sds((n * rows, cols), bf16),) * 2,
            in_specs=[VMEM] * 3,
            out_specs=(HBM,) * 10,
            scratch_shapes=[dma((3,))],
            compiler_params=pltpu.CompilerParams(vmem_limit_bytes=24 << 20),
        )(*held)

    split, column = P("fs", "tp"), P(None, "tp")
    return jax.shard_map(
        body,
        mesh=mesh,
        in_specs=(P("fs", None),) + (split,) * 4 + (P(),) * 2 + (column,) * 4,
        out_specs=(split,) * 4 + (column,) * 6,
        check_vma=False,
    )
```
